256 devices in a mesh: grp: 2 (over y), sp: 32 (over z, core), tp: 4 (over x).
Axes of the slice: x: 4, y: 2, z: 16, core: 2. Of those that a mesh axis runs over, the one named last changes fastest.
The devices are a block of a 4x16x16 slice.
Arguments:
- query_rows: bfloat16 [8192, 1024], P(('grp', 'sp'), 'tp'), parts along dimension 0, may hold values from -6 to 6
- key_rows: bfloat16 [8192, 1024], P(('grp', 'sp'), 'tp'), parts along dimension 0, may hold values from -6 to 6
- value_rows: bfloat16 [8192, 1024], P(('grp', 'sp'), 'tp'), parts along dimension 0, may hold values from -6 to 6
- gate_rows: bfloat16 [8192, 1024], P(('grp', 'sp'), 'tp'), parts along dimension 0, may hold values from -6 to 6
- log_decay: float32 [2, 8, 8192], P(None, 'tp', ('grp', 'sp')), parts along dimension 2, may hold values from -2 to 0, as said below
- head_gain: float32 [2, 1024], P(None, 'tp'), may hold values from 0.1 to 1.9
- out_weight: bfloat16 [1024, 2048], P('tp'), may hold values from -0.1875 to 0.1875
- residual: bfloat16 [8192, 2048], P(('grp', 'sp')), parts along dimension 0, may hold values from -6 to 6
- norm_gain: bfloat16 [2048], replicated, may hold values from 0.099609375 to 1.8984375
- gate_weight: bfloat16 [2048, 5632], P('sp', 'tp'), may hold values from -0.125 to 0.125
- up_weight: bfloat16 [2048, 5632], P('sp', 'tp'), may hold values from -0.125 to 0.125
- down_weight: bfloat16 [2048, 5632], P('sp', 'tp'), may hold values from -0.078125 to 0.078125
- gate_taps: bfloat16 [3, 5632], P(None, 'tp'), may hold values from -3.5 to 3.5
- up_taps: bfloat16 [3, 5632], P(None, 'tp'), may hold values from -3.5 to 3.5
Outputs:
- block_out: bfloat16 [8192, 2048], P(('grp', 'sp', 'tp')), parts along dimension 0
The draws below stay inside these ranges and needn't reach their ends.
There are 2 independent parts, one for each index of `grp`. The reference program is written for one: setup_inputs(seed, part) draws one part's arguments, and reference() takes and returns one part's arrays. A program takes and returns all parts, laid end to end along the dimension named above; an argument that names none is the same for every part. Nothing has to cross between parts.
Inputs may be any that keep to these rules, and one draw needn't show every extreme that they name: `log_decay`: every entry is negative.
All inputs are finite; a program needn't handle non-finite values.
Results may differ from the reference program's by a relative error of at most 0.017.
Values may be sent and summed in bfloat16 or wider, within the bound.
No kernel may reach another device: no remote copies, remote signals or barrier semaphores. Data moves between devices by JAX's collectives and lax.ppermute only.
A program may use at most 64 MiB of HBM per device.

```python
import math
import jax
import jax.numpy as jnp
from jax import lax

D = 2048
RETENTION_HEADS = 8
HEAD = 128
FF = 5632
TOK_DEV = 128
VALUE = 1024
TOKENS = 4096


def spread_log(subkey, shape, low_end, high_end):
    return jnp.exp(jax.random.uniform(subkey, shape, jnp.float32, jnp.log(low_end), jnp.log(high_end)))


def draw_log_decay(key, part):
    random_subkeys = jax.random.split(jax.random.fold_in(key, 17), 7)
    blocks = TOKENS // TOK_DEV
    slow_share = 0.5
    totals = spread_log(random_subkeys[1], (2, RETENTION_HEADS, 1), 0.2, 0.7)
    is_slow = jax.random.bernoulli(random_subkeys[0], slow_share, (2, RETENTION_HEADS, 1))
    reach_len = spread_log(random_subkeys[2], (2, RETENTION_HEADS, 1), 30.0, 100.0)
    baseline_decay_rate = jnp.where(is_slow, -totals / TOKENS, -1.0 / reach_len)
    multiplier = spread_log(random_subkeys[3], (2, RETENTION_HEADS, blocks, 1), 0.5, 1.5)
    multiplier = jnp.broadcast_to(multiplier, (2, RETENTION_HEADS, blocks, TOK_DEV)).reshape(2, RETENTION_HEADS, TOKENS)
    approximate_multiplier = jax.random.uniform(random_subkeys[4], (2, RETENTION_HEADS, TOKENS), jnp.float32, 0.6, 1.4)
    target_locations = jax.random.randint(random_subkeys[5], (2, RETENTION_HEADS, 2, 1), 0, TOKENS)
    spike_depth = jnp.log(jax.random.uniform(random_subkeys[6], (2, RETENTION_HEADS, 2, 1), jnp.float32, 0.55, 0.8))
    token_positions = jnp.arange(TOKENS)[None, None, None, :]
    spike_events = jnp.sum(jnp.where(token_positions == target_locations, spike_depth, 0.0), axis=2)
    return (baseline_decay_rate * multiplier * approximate_multiplier + spike_events).astype(jnp.float32)


def block_levels(key, shape, pieces, low, high):
    level, own = 1.0, jax.random.fold_in(key, 6)
    for position, blocks in pieces:
        draws = jnp.exp(jax.random.uniform(jax.random.fold_in(own, position), (blocks,), jnp.float32, low / len(pieces), high / len(pieces)))
        level = level * jnp.repeat(draws, shape[position] // blocks).reshape([-1 if axis == position else 1 for axis in range(len(shape))])
    return level


def normal_values(key, extent, scale, bound, cuts=(), dtype=jnp.bfloat16):
    entries = jax.random.normal(key, extent, jnp.float32) * scale
    if len(cuts) > 0:
        entries = block_levels(key, extent, cuts, -0.22, 0.18) * entries
    return jnp.clip(entries, min=-bound, max=bound).astype(dtype)


def setup_inputs(seed: int = 0, part: int = 0) -> dict:
    splits = jax.random.split(jax.random.key(seed), 15)
    part_keys = jax.random.split(jax.random.fold_in(splits[14], part), 15)
    query_rows = normal_values(part_keys[0], (TOKENS, VALUE), 1.0, 6.0, ((0, 32), (1, 4)))
    key_rows = normal_values(part_keys[1], (TOKENS, VALUE), 1.0, 6.0, ((0, 32), (1, 4)))
    value_rows = normal_values(part_keys[2], (TOKENS, VALUE), 1.0, 6.0, ((0, 32), (1, 4)))
    gate_rows = normal_values(part_keys[3], (TOKENS, VALUE), 1.0, 6.0, ((0, 32), (1, 4)))
    log_decay = draw_log_decay(jax.random.fold_in(jax.random.fold_in(splits[14], part), 71), part)
    head_gain = jnp.clip(1.0 + 0.18 * jax.random.normal(splits[5], (2, VALUE), jnp.float32), 0.1, 1.9)
    out_weight = normal_values(splits[6], (VALUE, D), VALUE ** -0.5, 0.1875, ((0, 4),))
    residual = normal_values(part_keys[7], (TOKENS, D), 1.0, 6.0, ((0, 32),))
    norm_gain = jnp.clip(1.0 + 0.18 * jax.random.normal(splits[8], (D,), jnp.float32), 0.099609375, 1.8984375).astype(jnp.bfloat16)
    gate_weight = normal_values(splits[9], (D, FF), D ** -0.5, 0.125, ((0, 32), (1, 4)))
    up_weight = normal_values(splits[10], (D, FF), D ** -0.5, 0.125, ((0, 32), (1, 4)))
    down_weight = normal_values(splits[11], (D, FF), FF ** -0.5, 0.078125, ((0, 32), (1, 4)))
    gate_taps = normal_values(splits[12], (3, FF), 3 ** -0.5, 3.5, ((1, 4),))
    up_taps = normal_values(splits[13], (3, FF), 3 ** -0.5, 3.5, ((1, 4),))
    return {"query_rows": query_rows, "key_rows": key_rows, "value_rows": value_rows, "gate_rows": gate_rows, "log_decay": log_decay, "head_gain": head_gain, "out_weight": out_weight, "residual": residual, "norm_gain": norm_gain, "gate_weight": gate_weight, "up_weight": up_weight, "down_weight": down_weight, "gate_taps": gate_taps, "up_taps": up_taps}


FULL_PRECISION = lax.Precision.HIGHEST
GROUP_EPS = 1e-05
NORM_EPS = 1e-06

def scan_retention(query_all, key_all, value_all, log_rates):
    length, head_count, head_width = query_all.shape
    block_len = math.gcd(length, 512)
    block_count = length // block_len
    query_blocks = query_all.reshape(block_count, block_len, head_count, head_width)
    key_blocks = key_all.reshape(block_count, block_len, head_count, head_width)
    value_blocks = value_all.reshape(block_count, block_len, head_count, head_width)
    rate_blocks = log_rates.T.reshape(block_count, block_len, head_count)
    lower_mask = jnp.arange(block_len)[:, None] >= jnp.arange(block_len)[None, :]

    def block_step(carry_state, inputs):
        query_blk, key_blk, value_blk, rate_blk = inputs
        cumul = jnp.cumsum(rate_blk, axis=0)
        gap_logs = cumul[:, None, :] - cumul[None, :, :]
        decay_mask = jnp.where(lower_mask[:, :, None], jnp.exp(jnp.minimum(gap_logs, 0.0)), 0.0)
        scores = jnp.einsum('thd,shd->tsh', query_blk, key_blk, precision=FULL_PRECISION) * decay_mask
        inner_part = jnp.einsum('tsh,she->the', scores, value_blk, precision=FULL_PRECISION)
        carried = jnp.einsum('thd,hde->the', query_blk * jnp.exp(cumul)[:, :, None], carry_state, precision=FULL_PRECISION)
        last_cumul = cumul[-1]
        key_decayed = key_blk * jnp.exp(last_cumul[None, :] - cumul)[:, :, None]
        new_state = carry_state * jnp.exp(last_cumul)[:, None, None] + jnp.einsum('shd,she->hde', key_decayed, value_blk, precision=FULL_PRECISION)
        return (new_state, inner_part + carried)
    zero_state = jnp.zeros((head_count, head_width, head_width), jnp.float32)
    ignored, block_outs = lax.scan(block_step, zero_state, (query_blocks, key_blocks, value_blocks, rate_blocks))
    return block_outs.reshape(length, head_count, head_width)

def group_norm(values):
    length, head_count, head_width = values.shape
    centre = values - lax.optimization_barrier(jnp.mean(values, axis=2, keepdims=True))
    spread = lax.optimization_barrier(jnp.mean(centre * centre, axis=2, keepdims=True))
    return (centre * lax.rsqrt(spread + GROUP_EPS)).reshape(length, head_count * head_width)

def rms_scale(middle, gain):
    values = middle.astype(jnp.float32)
    multiplier = lax.rsqrt(lax.optimization_barrier(jnp.mean(values * values, axis=1, keepdims=True)) + NORM_EPS)
    return (values * multiplier * gain.astype(jnp.float32)).astype(jnp.bfloat16)

def reference(query_rows, key_rows, value_rows, gate_rows, log_decay, head_gain, out_weight, residual, norm_gain, gate_weight, up_weight, down_weight, gate_taps, up_taps):
    key_scale = HEAD ** (-0.5)
    query_all = query_rows.astype(jnp.float32).reshape(TOKENS, RETENTION_HEADS, HEAD)
    key_all = key_rows.astype(jnp.float32).reshape(TOKENS, RETENTION_HEADS, HEAD) * key_scale
    value_all = value_rows.astype(jnp.float32).reshape(TOKENS, RETENTION_HEADS, HEAD)
    ahead_out = scan_retention(query_all, key_all, value_all, log_decay[0])
    behind_out = scan_retention(query_all[::-1], key_all[::-1], value_all[::-1], log_decay[1][:, ::-1])[::-1]
    combined = group_norm(ahead_out) * head_gain[0] + group_norm(behind_out) * head_gain[1]
    mixed_heads = (jax.nn.silu(gate_rows.astype(jnp.float32)) * combined).astype(jnp.bfloat16)
    attended = jnp.dot(mixed_heads, out_weight, preferred_element_type=jnp.float32)
    middle = lax.optimization_barrier((residual.astype(jnp.float32) + attended).astype(jnp.bfloat16))
    normed = rms_scale(middle, norm_gain)
    model_width = normed.shape[1]
    zero_row = jnp.zeros((1, model_width), jnp.bfloat16)
    padded = jnp.concatenate([zero_row, normed, zero_row], axis=0)
    block_len = math.gcd(TOKENS, 512)
    taps_gate = gate_taps.astype(jnp.float32)
    taps_up = up_taps.astype(jnp.float32)

    def one_block(block_index):
        first_row = (block_index * block_len).astype(jnp.int32)
        rows_with_rims = lax.dynamic_slice_in_dim(padded, first_row, block_len + 2, 0)
        pre_gate = lax.optimization_barrier(jnp.dot(rows_with_rims, gate_weight, preferred_element_type=jnp.float32).astype(jnp.bfloat16)).astype(jnp.float32)
        pre_up = lax.optimization_barrier(jnp.dot(rows_with_rims, up_weight, preferred_element_type=jnp.float32).astype(jnp.bfloat16)).astype(jnp.float32)
        conv_gate = taps_gate[0] * pre_gate[:-2] + taps_gate[1] * pre_gate[1:-1] + taps_gate[2] * pre_gate[2:]
        conv_up = taps_up[0] * pre_up[:-2] + taps_up[1] * pre_up[1:-1] + taps_up[2] * pre_up[2:]
        hidden = (jax.nn.silu(conv_gate) * conv_up).astype(jnp.bfloat16)
        ff_out = lax.dot_general(hidden, down_weight, (((1,), (1,)), ((), ())), preferred_element_type=jnp.float32)
        middle_rows = lax.dynamic_slice_in_dim(middle, first_row, block_len, 0).astype(jnp.float32)
        return (middle_rows + ff_out).astype(jnp.bfloat16)
    block_outs = lax.map(one_block, jnp.arange(TOKENS // block_len).astype(jnp.int32))
    return block_outs.reshape(TOKENS, model_width)
```

```python
import math

import jax
import jax.numpy as jnp
from jax import lax
from jax.experimental import pallas as pl
from jax.experimental.pallas import tpu as pltpu
from jax.sharding import Mesh
from jax.sharding import PartitionSpec as P

HEAD = 128
LANES = 128
SP = ("z", "c")
ROWS = ("pg", "pr", "z", "c")
PEERS = ("pr", "tp")

GROUP_EPS = 1e-05
NORM_EPS = 1e-06

F32 = jnp.float32
BF16 = jnp.bfloat16
VMEM = pl.BlockSpec(memory_space=pltpu.VMEM)


def call(body, outs, *args):
    return pl.pallas_call(
        body,
        out_shape=outs,
        in_specs=[VMEM] * len(args),
        out_specs=jax.tree.map(lambda _: VMEM, outs),
    )(*args)


def shaped(shape, dtype):
    return jax.ShapeDtypeStruct(shape, dtype)


def dot(a, b, dims=((1,), (0,))):
    return lax.dot_general(a, b, (dims, ((), ())), preferred_element_type=F32)


def split_columns(pair, width):
    tiles = width // LANES
    share = -(-tiles // pair)
    step = (tiles - share) // (pair - 1) if pair > 1 else 0
    return share * LANES, step * LANES


def pick_weights(pair, gate_ref, up_ref, down_ref, out_ref):
    cols, step = split_columns(pair, gate_ref.shape[1])
    start = pl.multiple_of(lax.axis_index("pr") * step, LANES)
    for i, ref in enumerate((gate_ref, up_ref, down_ref)):
        out_ref[:, i * cols : (i + 1) * cols] = ref[:, pl.ds(start, cols)]


def local_retention(q_ref, k_ref, v_ref, rate_ref, inner_ref, query_ref, keep_ref, send_ref):
    n, width = q_ref.shape
    heads = width // HEAD
    row = lax.broadcasted_iota(jnp.int32, (n, n), 0)
    col = lax.broadcasted_iota(jnp.int32, (n, n), 1)
    scale = HEAD ** (-0.5)
    first = lax.axis_index("c") == 0
    for h in range(heads):
        cut = slice(h * HEAD, (h + 1) * HEAD)
        q, k, v = q_ref[:, cut], k_ref[:, cut], v_ref[:, cut]
        scores = dot(q, k, ((1,), (1,))) * scale
        states, decays = [], []
        for way in range(2):
            rate = rate_ref[way, h : h + 1, :]
            rate_col = jnp.sum(jnp.where(row == col, rate, 0.0), axis=1, keepdims=True)
            seen = col <= row if way == 0 else col >= row
            seen_by = row <= col if way == 0 else row >= col
            total_col = jnp.sum(jnp.where(seen, rate, 0.0), axis=1, keepdims=True)
            total_row = jnp.sum(jnp.where(seen_by, rate_col, 0.0), axis=0, keepdims=True)
            whole = jnp.sum(rate, axis=1, keepdims=True)
            mask = jnp.where(seen, jnp.exp(jnp.minimum(total_col - total_row, 0.0)), 0.0)
            inner_ref[way, :, cut] = dot((scores * mask).astype(BF16), v)
            query_ref[way, :, cut] = (q.astype(F32) * jnp.exp(total_col)).astype(BF16)
            weight = jnp.exp(whole - total_col) * scale
            states.append(dot((k.astype(F32) * weight).astype(BF16), v, ((0,), (0,))))
            decays.append(jnp.broadcast_to(jnp.exp(whole), (1, HEAD)))
        rows = slice(h * HEAD, (h + 1) * HEAD)
        keep_ref[rows, :] = jnp.where(first, states[0], states[1])
        send_ref[rows, :] = jnp.where(first, states[1], states[0])
        mark = slice(heads * HEAD + h, heads * HEAD + h + 1)
        keep_ref[mark, :] = jnp.where(first, decays[0], decays[1])
        send_ref[mark, :] = jnp.where(first, decays[1], decays[0])


def pack_states(keep_ref, got_ref, out_ref):
    pieces = out_ref.shape[0]
    heads = keep_ref.shape[0] // HEAD
    rows = HEAD // pieces
    marks = []
    for h in range(heads):
        at = heads * HEAD + h
        a = keep_ref[at : at + 1, :] * got_ref[at : at + 1, :]
        high = a.astype(BF16).astype(F32)
        middle = (a - high).astype(BF16).astype(F32)
        low = a - high - middle
        marks += [high, middle, low]
    used = heads * rows
    marks.append(jnp.zeros((out_ref.shape[1] - used - len(marks), LANES), F32))
    marks = jnp.concatenate(marks, axis=0).astype(BF16)
    for z in range(pieces):
        parts = []
        for h in range(heads):
            at = heads * HEAD + h
            cut = slice(h * HEAD + z * rows, h * HEAD + (z + 1) * rows)
            parts.append(keep_ref[cut, :] * got_ref[at : at + 1, :] + got_ref[cut, :])
        out_ref[z, 0:used, :] = jnp.concatenate(parts, axis=0).astype(BF16)
        out_ref[z, used:, :] = marks


def scan_states(in_ref, out_ref):
    pieces, used, _ = out_ref.shape
    first = lax.axis_index("c") == 0
    half = used // 2
    state = jnp.zeros((used, LANES), F32)
    for t in range(pieces):
        j = jnp.where(first, t, pieces - 1 - t)
        part = in_ref[j].astype(F32)
        out_ref[j] = state.astype(BF16)
        decay = [
            jnp.sum(part[used + 3 * h : used + 3 * h + 3, :], axis=0, keepdims=True)
            for h in range(2)
        ]
        decay = jnp.concatenate([jnp.broadcast_to(d, (half, LANES)) for d in decay], axis=0)
        state = state * decay + part[:used, :]


def spread_states(in_ref, keep_ref, own_ref, send_ref):
    pieces, used, _ = in_ref.shape
    heads = own_ref.shape[0] // HEAD
    rows = used // heads
    for h in range(heads):
        at = heads * HEAD + h
        state = jnp.concatenate(
            [in_ref[z].astype(F32)[h * rows : (h + 1) * rows, :] for z in range(pieces)], axis=0
        )
        cut = slice(h * HEAD, (h + 1) * HEAD)
        own_ref[cut, :] = state.astype(BF16)
        send_ref[cut, :] = (state * keep_ref[at : at + 1, :] + keep_ref[cut, :]).astype(BF16)


def group_norm(values):
    centre = values - jnp.mean(values, axis=1, keepdims=True)
    spread = jnp.mean(centre * centre, axis=1, keepdims=True)
    return centre * lax.rsqrt(spread + GROUP_EPS)


def mix(inner_ref, query_ref, own_ref, got_ref, gate_ref, gain_ref, weight_ref, out_ref):
    heads = gate_ref.shape[1] // HEAD
    first = lax.axis_index("c") == 0
    mixed = []
    for h in range(heads):
        cut = slice(h * HEAD, (h + 1) * HEAD)
        own, got = own_ref[cut, :], got_ref[cut, :]
        combined = 0.0
        for way in range(2):
            state = jnp.where(first, own, got) if way == 0 else jnp.where(first, got, own)
            values = inner_ref[way, :, cut] + dot(query_ref[way, :, cut], state)
            combined = combined + group_norm(values) * gain_ref[way : way + 1, cut]
        gate = gate_ref[:, cut].astype(F32)
        mixed.append((gate / (1.0 + jnp.exp(-gate)) * combined).astype(BF16))
    mixed = jnp.concatenate(mixed, axis=1)
    attended = dot(mixed, weight_ref[...]).astype(BF16)
    parts, rows, _ = out_ref.shape
    for p in range(parts):
        out_ref[p] = attended[p * rows : (p + 1) * rows, :]


def finish_middle(in_ref, residual_ref, gain_ref, middle_ref, out_ref):
    rows = middle_ref.shape[0]
    start = pl.multiple_of(lax.axis_index("tp") * rows, rows)
    attended = jnp.sum(in_ref[...].astype(F32), axis=0)
    middle = (residual_ref[pl.ds(start, rows), :].astype(F32) + attended).astype(BF16)
    middle_ref[...] = middle
    values = middle.astype(F32)
    scale = lax.rsqrt(jnp.mean(values * values, axis=1, keepdims=True) + NORM_EPS)
    normed = (values * scale * gain_ref[...].astype(F32)).astype(BF16)
    for p in range(out_ref.shape[0]):
        out_ref[p] = normed


def convolved(pre, halo, taps, pair):
    n = pre.shape[0] // pair
    row = lax.broadcasted_iota(jnp.int32, (n, pre.shape[1]), 0)
    spans = []
    for s in range(pair):
        x = pre[s * n : (s + 1) * n, :]
        before = jnp.where(row == 0, halo[s : s + 1, :], pltpu.roll(x, 1, 0))
        after = jnp.where(row == n - 1, halo[pair + s : pair + s + 1, :], pltpu.roll(x, n - 1, 0))
        spans.append(taps[0:1] * before + taps[1:2] * x + taps[2:3] * after)
    return jnp.concatenate(spans, axis=0)


def feed_forward(
    pair, x_ref, halo_ref, gate_ref, up_ref, down_ref, gt_ref, ut_ref, out_ref, acc_ref
):
    j = pl.program_id(0)
    block = gate_ref.shape[1]
    cols, step = split_columns(pair, gt_ref.shape[1])
    member = lax.axis_index("pr")
    at = pl.multiple_of(member * step + j * block, LANES)
    column = at + lax.broadcasted_iota(jnp.int32, (1, block), 1)
    x, halo = x_ref[...], halo_ref[...]

    def branch(weight, taps):
        pre = dot(x, weight).astype(BF16).astype(F32)
        edge = dot(halo, weight).astype(BF16).astype(F32)
        return convolved(pre, edge, taps, pair)

    gate = branch(gate_ref[...], gt_ref[:, pl.ds(at, block)].astype(F32))
    taps = jnp.where(column >= member * cols, ut_ref[:, pl.ds(at, block)].astype(F32), 0.0)
    up = branch(up_ref[...], taps)
    hidden = (gate / (1.0 + jnp.exp(-gate)) * up).astype(BF16)
    part = dot(hidden, down_ref[...], ((1,), (1,)))

    @pl.when(j == 0)
    def _():
        acc_ref[...] = part

    @pl.when(j > 0)
    def _():
        acc_ref[...] += part

    @pl.when(j == pl.num_programs(0) - 1)
    def _():
        parts, rows, _ = out_ref.shape
        for p in range(parts):
            out_ref[p] = acc_ref[p * rows : (p + 1) * rows, :].astype(BF16)


def run_feed_forward(pair, peers, normed, halo, gathered, gate_taps, up_taps):
    depth, columns = gathered.shape
    cols = columns // 3
    block = 256
    steps = cols // block
    whole = lambda a: pl.BlockSpec(a.shape, lambda j: (0,) * a.ndim)
    piece = lambda i: pl.BlockSpec((depth, block), lambda j, i=i: (0, i * steps + j))
    rows = normed.shape[0]
    return pl.pallas_call(
        lambda *refs: feed_forward(pair, *refs),
        grid=(steps,),
        out_shape=shaped((peers, rows // peers, depth), BF16),
        in_specs=[whole(normed), whole(halo), piece(0), piece(1), piece(2)]
        + [whole(gate_taps), whole(up_taps)],
        out_specs=pl.BlockSpec((peers, rows // peers, depth), lambda j: (0, 0, 0)),
        scratch_shapes=[pltpu.VMEM((rows, depth), F32)],
    )(normed, halo, gathered, gathered, gathered, gate_taps, up_taps)


def across(x, axes):
    return lax.all_to_all(x, axes, 0, 0, tiled=True)


def shards(
    query_rows,
    key_rows,
    value_rows,
    gate_rows,
    log_decay,
    head_gain,
    out_weight,
    residual,
    norm_gain,
    gate_weight,
    up_weight,
    down_weight,
    gate_taps,
    up_taps,
):
    pair, chips, tp = lax.axis_size("pr"), lax.axis_size("z"), lax.axis_size("tp")
    peers = pair * tp
    rows, width = query_rows.shape
    depth = residual.shape[1]
    heads = width // HEAD
    cols, _ = split_columns(pair, gate_weight.shape[1])

    picked = call(
        lambda *refs: pick_weights(pair, *refs),
        shaped((gate_weight.shape[0], 3 * cols), BF16),
        gate_weight,
        up_weight,
        down_weight,
    )
    gathered = lax.all_gather(picked, SP, axis=0, tiled=True)

    marked = shaped((heads * HEAD + 8, HEAD), F32)
    inner, query, keep, send = call(
        local_retention,
        (shaped((2, rows, width), F32), shaped((2, rows, width), BF16), marked, marked),
        query_rows,
        key_rows,
        value_rows,
        log_decay,
    )
    swap = [(0, 1), (1, 0)]
    got = lax.ppermute(send, "c", swap)
    used = heads * HEAD // chips
    message = call(pack_states, shaped((chips, used + 16, HEAD), BF16), keep, got)
    prefix = call(scan_states, shaped((chips, used, HEAD), BF16), across(message, "z"))
    state = shaped((heads * HEAD, HEAD), BF16)
    own, other = call(spread_states, (state, state), across(prefix, "z"), keep)
    entering = lax.ppermute(other, "c", swap)
    attended = call(
        mix,
        shaped((tp, rows // tp, depth), BF16),
        inner,
        query,
        own,
        entering,
        gate_rows,
        head_gain,
        out_weight,
    )
    middle, copies = call(
        finish_middle,
        (shaped((rows // tp, depth), BF16), shaped((peers, rows // tp, depth), BF16)),
        across(attended, "tp"),
        residual,
        norm_gain.reshape(1, depth),
    )
    normed = across(copies, PEERS).reshape(pair, rows, depth)
    size = lax.axis_size("z") * lax.axis_size("c")
    onward = [(i, i + 1) for i in range(size - 1)]
    back = [(j, i) for i, j in onward]
    before = lax.ppermute(normed[:, rows - 1], SP, onward)
    after = lax.ppermute(normed[:, 0], SP, back)
    fill = jnp.zeros((16 - 2 * pair, depth), BF16)
    halo = jnp.concatenate([before, after, fill], axis=0)
    parts = run_feed_forward(
        pair, peers, normed.reshape(pair * rows, depth), halo, gathered, gate_taps, up_taps
    )
    summed = across(parts, PEERS).astype(F32).sum(axis=0)
    return (middle.astype(F32) + summed).astype(BF16)


def solution(mesh):
    groups, tp = mesh.shape["grp"], mesh.shape["tp"]
    pair = math.gcd(groups, 2)
    split = Mesh(
        mesh.devices.reshape(groups // pair, pair, mesh.shape["sp"] // 2, 2, tp),
        ("pg", "pr", "z", "c", "tp"),
    )
    placed = (
        P(ROWS, "tp"),
        P(ROWS, "tp"),
        P(ROWS, "tp"),
        P(ROWS, "tp"),
        P(None, "tp", ROWS),
        P(None, "tp"),
        P("tp", None),
        P(ROWS, None),
        P(),
        P(SP, "tp"),
        P(SP, "tp"),
        P(SP, "tp"),
        P(None, "tp"),
        P(None, "tp"),
    )
    return jax.shard_map(
        shards, mesh=split, in_specs=placed, out_specs=P((*ROWS, "tp"), None), check_vma=False
    )
```

```python
import math

import jax
import jax.numpy as jnp
from jax import lax
from jax.experimental import pallas as pl
from jax.experimental.pallas import tpu as pltpu
from jax.sharding import Mesh
from jax.sharding import PartitionSpec as P

HEAD = 128
LANES = 128
SP = ("z", "c")
ROWS = ("pg", "pr", "z", "c")
PEERS = ("pr", "tp")

GROUP_EPS = 1e-05
NORM_EPS = 1e-06

F32 = jnp.float32
BF16 = jnp.bfloat16
VMEM = pl.BlockSpec(memory_space=pltpu.VMEM)
HBM = pl.BlockSpec(memory_space=pl.ANY)


def call(body, outs, *args, limit=12, **more):
    spec = {"in_specs": [VMEM] * len(args), "out_specs": jax.tree.map(lambda _: VMEM, outs)}
    return pl.pallas_call(
        body,
        out_shape=outs,
        compiler_params=pltpu.CompilerParams(vmem_limit_bytes=limit << 20),
        **{**spec, **more},
    )(*args)


def shaped(shape, dtype):
    return jax.ShapeDtypeStruct(shape, dtype)


def dot(a, b, dims=((1,), (0,))):
    return lax.dot_general(a, b, (dims, ((), ())), preferred_element_type=F32)


def split_columns(pair, width):
    tiles = width // LANES
    share = -(-tiles // pair)
    step = (tiles - share) // (pair - 1) if pair > 1 else 0
    return share * LANES, step * LANES


def pick_weights(pair, gate_ref, up_ref, down_ref, out_ref, sems):
    cols, step = split_columns(pair, gate_ref.shape[1])
    start = pl.multiple_of(lax.axis_index("pr") * step, LANES)
    copies = [
        pltpu.make_async_copy(
            ref.at[:, pl.ds(start, cols)], out_ref.at[:, pl.ds(i * cols, cols)], sems.at[i]
        )
        for i, ref in enumerate((gate_ref, up_ref, down_ref))
    ]
    for copy in copies:
        copy.start()
    for copy in copies:
        copy.wait()


def local_retention(
    q_ref,
    k_ref,
    v_ref,
    rate_ref,
    weight_ref,
    inner_ref,
    query_ref,
    keep_ref,
    send_ref,
    half_ref,
    sem,
):
    half = half_ref.shape[0]
    start = pl.multiple_of(lax.axis_index("c") * half, half)
    copy = pltpu.make_async_copy(weight_ref.at[pl.ds(start, half), :], half_ref, sem)
    copy.start()
    n, width = q_ref.shape
    heads = width // HEAD
    row = lax.broadcasted_iota(jnp.int32, (n, n), 0)
    col = lax.broadcasted_iota(jnp.int32, (n, n), 1)
    scale = HEAD ** (-0.5)
    first = lax.axis_index("c") == 0
    for h in range(heads):
        cut = slice(h * HEAD, (h + 1) * HEAD)
        q, k, v = q_ref[:, cut], k_ref[:, cut], v_ref[:, cut]
        scores = dot(q, k, ((1,), (1,))) * scale
        states, decays = [], []
        for way in range(2):
            rate = rate_ref[way, h : h + 1, :]
            rate_col = jnp.sum(jnp.where(row == col, rate, 0.0), axis=1, keepdims=True)
            seen = col <= row if way == 0 else col >= row
            seen_by = row <= col if way == 0 else row >= col
            total_col = jnp.sum(jnp.where(seen, rate, 0.0), axis=1, keepdims=True)
            total_row = jnp.sum(jnp.where(seen_by, rate_col, 0.0), axis=0, keepdims=True)
            whole = jnp.sum(rate, axis=1, keepdims=True)
            mask = jnp.where(seen, jnp.exp(jnp.minimum(total_col - total_row, 0.0)), 0.0)
            inner_ref[way, :, cut] = dot((scores * mask).astype(BF16), v)
            query_ref[way, :, cut] = (q.astype(F32) * jnp.exp(total_col)).astype(BF16)
            weight = jnp.exp(whole - total_col) * scale
            states.append(dot((k.astype(F32) * weight).astype(BF16), v, ((0,), (0,))))
            decays.append(jnp.broadcast_to(jnp.exp(whole), (1, HEAD)))
        rows = slice(h * HEAD, (h + 1) * HEAD)
        keep_ref[rows, :] = jnp.where(first, states[0], states[1])
        send_ref[rows, :] = jnp.where(first, states[1], states[0])
        mark = slice(heads * HEAD + h, heads * HEAD + h + 1)
        keep_ref[mark, :] = jnp.where(first, decays[0], decays[1])
        send_ref[mark, :] = jnp.where(first, decays[1], decays[0])
    copy.wait()


def pack_states(keep_ref, got_ref, out_ref):
    pieces = out_ref.shape[0]
    heads = keep_ref.shape[0] // HEAD
    rows = HEAD // pieces
    marks = []
    for h in range(heads):
        at = heads * HEAD + h
        a = keep_ref[at : at + 1, :] * got_ref[at : at + 1, :]
        high = a.astype(BF16).astype(F32)
        middle = (a - high).astype(BF16).astype(F32)
        low = a - high - middle
        marks += [high, middle, low]
    used = heads * rows
    marks.append(jnp.zeros((out_ref.shape[1] - used - len(marks), LANES), F32))
    marks = jnp.concatenate(marks, axis=0).astype(BF16)
    for z in range(pieces):
        parts = []
        for h in range(heads):
            at = heads * HEAD + h
            cut = slice(h * HEAD + z * rows, h * HEAD + (z + 1) * rows)
            parts.append(keep_ref[cut, :] * got_ref[at : at + 1, :] + got_ref[cut, :])
        out_ref[z, 0:used, :] = jnp.concatenate(parts, axis=0).astype(BF16)
        out_ref[z, used:, :] = marks


def scan_states(in_ref, out_ref):
    pieces, used, _ = out_ref.shape
    first = lax.axis_index("c") == 0
    half = used // 2
    state = jnp.zeros((used, LANES), F32)
    for t in range(pieces):
        j = jnp.where(first, t, pieces - 1 - t)
        part = in_ref[j].astype(F32)
        out_ref[j] = state.astype(BF16)
        decay = [
            jnp.sum(part[used + 3 * h : used + 3 * h + 3, :], axis=0, keepdims=True)
            for h in range(2)
        ]
        decay = jnp.concatenate([jnp.broadcast_to(d, (half, LANES)) for d in decay], axis=0)
        state = state * decay + part[:used, :]


def spread_states(in_ref, keep_ref, own_ref, send_ref):
    pieces, used, _ = in_ref.shape
    heads = own_ref.shape[0] // HEAD
    rows = used // heads
    for h in range(heads):
        at = heads * HEAD + h
        state = jnp.concatenate(
            [in_ref[z].astype(F32)[h * rows : (h + 1) * rows, :] for z in range(pieces)], axis=0
        )
        cut = slice(h * HEAD, (h + 1) * HEAD)
        own_ref[cut, :] = state.astype(BF16)
        send_ref[cut, :] = (state * keep_ref[at : at + 1, :] + keep_ref[cut, :]).astype(BF16)


def group_norm(values):
    centre = values - jnp.mean(values, axis=1, keepdims=True)
    spread = jnp.mean(centre * centre, axis=1, keepdims=True)
    return centre * lax.rsqrt(spread + GROUP_EPS)


def mix(inner_ref, query_ref, own_ref, got_ref, gate_ref, gain_ref, out_ref):
    heads = gate_ref.shape[1] // HEAD
    first = lax.axis_index("c") == 0
    mixed = []
    for h in range(heads):
        cut = slice(h * HEAD, (h + 1) * HEAD)
        own, got = own_ref[cut, :], got_ref[cut, :]
        combined = 0.0
        for way in range(2):
            state = jnp.where(first, own, got) if way == 0 else jnp.where(first, got, own)
            values = inner_ref[way, :, cut] + dot(query_ref[way, :, cut], state)
            combined = combined + group_norm(values) * gain_ref[way : way + 1, cut]
        gate = gate_ref[:, cut].astype(F32)
        mixed.append((gate / (1.0 + jnp.exp(-gate)) * combined).astype(BF16))
    mixed = jnp.concatenate(mixed, axis=1)
    for p in range(out_ref.shape[0]):
        out_ref[p] = mixed


def project(pair, tp, *refs):
    mixed_ref, weight_ref, *refs = refs
    near, refs = refs[: tp - 1], refs[tp - 1 :]
    far, refs = refs[: tp - 1], refs[tp - 1 :]
    residuals, refs = refs[:pair], refs[pair:]
    gain_ref, normed_ref, middle_ref, first_ref, last_ref, scratch = refs
    me, member, core = lax.axis_index("tp"), lax.axis_index("pr"), lax.axis_index("c")
    n, width = mixed_ref.shape[1:]
    half = width // 2
    low = pl.multiple_of(core * half, half)
    high = pl.multiple_of((1 - core) * half, half)
    attended = 0.0
    for d in range(tp):
        parts = []
        for s in range(pair):
            i = lax.rem(member + s, pair) * tp + lax.rem(me - d + tp, tp)
            if d == 0:
                parts.append(mixed_ref[i])
            else:
                parts.append(
                    jnp.concatenate(
                        [mixed_ref[i, :, pl.ds(low, half)], mixed_ref[i, :, pl.ds(high, half)]],
                        axis=1,
                    )
                )
        rows = jnp.concatenate(parts, axis=0)
        if d == 0:
            weight = weight_ref[...]
        else:
            weight = jnp.concatenate([near[d - 1][...], far[d - 1][...]], axis=0)
        attended = attended + dot(rows, weight)
    firsts, lasts = [], []
    for s in range(pair):
        part = attended[s * n : (s + 1) * n, :]
        middle = (residuals[s][...].astype(F32) + part).astype(BF16)
        if s == 0:
            scratch[...] = middle
        values = middle.astype(F32)
        scale = lax.rsqrt(jnp.mean(values * values, axis=1, keepdims=True) + NORM_EPS)
        normed = values * scale * gain_ref[...].astype(F32)
        normed_ref[s * n : (s + 1) * n, :] = normed.astype(BF16)
        firsts.append(normed[0:1, :])
        lasts.append(normed[n - 1 : n, :])
    own = middle_ref.shape[0]
    middle_ref[...] = scratch[pl.ds(pl.multiple_of(me * own, own), own), :]
    fill = [jnp.zeros((first_ref.shape[0] - pair, first_ref.shape[1]), F32)]
    first_ref[...] = jnp.concatenate(firsts + fill, axis=0).astype(BF16)
    last_ref[...] = jnp.concatenate(lasts + fill, axis=0).astype(BF16)


def convolved(pre, pair, taps):
    n = (pre.shape[0] - 16) // pair
    row = lax.broadcasted_iota(jnp.int32, (n, pre.shape[1]), 0)
    spans = []
    for s in range(pair):
        x = pre[s * n : (s + 1) * n, :]
        at = pair * n + s
        before = jnp.where(row == 0, pre[at : at + 1, :], pltpu.roll(x, 1, 0))
        after = jnp.where(row == n - 1, pre[at + 8 : at + 9, :], pltpu.roll(x, n - 1, 0))
        spans.append(taps[0:1] * before + taps[1:2] * x + taps[2:3] * after)
    return jnp.concatenate(spans, axis=0)


def feed_forward(
    pair,
    tp,
    x_ref,
    before_ref,
    after_ref,
    gate_ref,
    up_ref,
    down_ref,
    gt_ref,
    ut_ref,
    out_ref,
    rows_ref,
    acc_ref,
):
    j = pl.program_id(0)
    block = gate_ref.shape[1]
    cols, step = split_columns(pair, gt_ref.shape[1])
    member = lax.axis_index("pr")
    at = pl.multiple_of(member * step + j * block, LANES)
    column = at + lax.broadcasted_iota(jnp.int32, (1, block), 1)
    count = x_ref.shape[0]

    @pl.when(j == 0)
    def _():
        rows_ref[0:count, :] = x_ref[...]
        rows_ref[count:, :] = jnp.concatenate([before_ref[...], after_ref[...]], axis=0)

    def branch(weight, taps):
        pre = dot(rows_ref[...], weight).astype(BF16).astype(F32)
        return convolved(pre, pair, taps)

    gate = branch(gate_ref[...], gt_ref[:, pl.ds(at, block)].astype(F32))
    taps = jnp.where(column >= member * cols, ut_ref[:, pl.ds(at, block)].astype(F32), 0.0)
    up = branch(up_ref[...], taps)
    hidden = (gate / (1.0 + jnp.exp(-gate)) * up).astype(BF16)
    part = dot(hidden, down_ref[...], ((1,), (1,)))
    last = pl.num_programs(0) - 1

    @pl.when(j == 0)
    def _():
        acc_ref[...] = part

    @pl.when((j > 0) & (j < last))
    def _():
        acc_ref[...] += part

    @pl.when(j == last)
    def _():
        rows = out_ref.shape[1]
        for s in range(pair):
            for q in range(tp):
                cut = slice((s * tp + q) * rows, (s * tp + q + 1) * rows)
                whole = acc_ref[cut, :] + part[cut, :] if cols > block else part[cut, :]
                out_ref[lax.rem(member + s, pair) * tp + q] = whole.astype(BF16)


def run_feed_forward(pair, tp, normed, before, after, gathered, gate_taps, up_taps):
    depth, columns = gathered.shape
    cols = columns // 3
    block = 256
    steps = cols // block
    whole = lambda a: pl.BlockSpec(a.shape, lambda j: (0,) * a.ndim)
    piece = lambda i: pl.BlockSpec((depth, block), lambda j, i=i: (0, i * steps + j))
    rows = normed.shape[0]
    out = (pair * tp, rows // (pair * tp), depth)
    return pl.pallas_call(
        lambda *refs: feed_forward(pair, tp, *refs),
        grid=(steps,),
        out_shape=shaped(out, BF16),
        in_specs=[whole(normed), whole(before), whole(after), piece(0), piece(1), piece(2)]
        + [whole(gate_taps), whole(up_taps)],
        out_specs=pl.BlockSpec(out, lambda j: (0, 0, 0)),
        scratch_shapes=[pltpu.VMEM((rows + 16, depth), BF16), pltpu.VMEM((rows, depth), F32)],
        compiler_params=pltpu.CompilerParams(vmem_limit_bytes=56 << 20),
    )(normed, before, after, gathered, gathered, gathered, gate_taps, up_taps)


def across(x, axes):
    return lax.all_to_all(x, axes, 0, 0, tiled=True)


def shards(
    query_rows,
    key_rows,
    value_rows,
    gate_rows,
    log_decay,
    head_gain,
    out_weight,
    residual,
    norm_gain,
    gate_weight,
    up_weight,
    down_weight,
    gate_taps,
    up_taps,
):
    pair, chips, tp = lax.axis_size("pr"), lax.axis_size("z"), lax.axis_size("tp")
    peers = pair * tp
    rows, width = query_rows.shape
    depth = residual.shape[1]
    heads = width // HEAD
    cols, _ = split_columns(pair, gate_weight.shape[1])

    picked = call(
        lambda *refs: pick_weights(pair, *refs),
        shaped((gate_weight.shape[0], 3 * cols), BF16),
        gate_weight,
        up_weight,
        down_weight,
        in_specs=[HBM] * 3,
        out_specs=HBM,
        scratch_shapes=[pltpu.SemaphoreType.DMA((3,))],
    )
    gathered = lax.all_gather(picked, SP, axis=0, tiled=True)

    marked = shaped((heads * HEAD + 8, HEAD), F32)
    inner, query, keep, send, half = call(
        local_retention,
        (
            shaped((2, rows, width), F32),
            shaped((2, rows, width), BF16),
            marked,
            marked,
            shaped((width // 2, depth), BF16),
        ),
        query_rows,
        key_rows,
        value_rows,
        log_decay,
        out_weight,
        in_specs=[VMEM] * 4 + [HBM],
        out_specs=(VMEM,) * 4 + (HBM,),
        scratch_shapes=[pltpu.SemaphoreType.DMA],
    )
    swap = [(0, 1), (1, 0)]
    got = lax.ppermute(send, "c", swap)
    near = [
        lax.ppermute(half, "tp", [(i, (i + d) % tp) for i in range(tp)]) for d in range(1, tp)
    ]
    far = [lax.ppermute(a, "c", swap) for a in near]
    residuals = [residual] + [
        lax.ppermute(residual, "pr", [((i + s) % pair, i) for i in range(pair)])
        for s in range(1, pair)
    ]
    used = heads * HEAD // chips
    message = call(pack_states, shaped((chips, used + 16, HEAD), BF16), keep, got)
    prefix = call(scan_states, shaped((chips, used, HEAD), BF16), across(message, "z"))
    state = shaped((heads * HEAD, HEAD), BF16)
    own, other = call(spread_states, (state, state), across(prefix, "z"), keep)
    entering = lax.ppermute(other, "c", swap)
    mixed = call(
        mix,
        shaped((peers, rows, width), BF16),
        inner,
        query,
        own,
        entering,
        gate_rows,
        head_gain,
    )
    edge = shaped((8, depth), BF16)
    normed, middle, first, last = call(
        lambda *refs: project(pair, tp, *refs),
        (shaped((pair * rows, depth), BF16), shaped((rows // tp, depth), BF16), edge, edge),
        across(mixed, PEERS),
        out_weight,
        *near,
        *far,
        *residuals,
        norm_gain.reshape(1, depth),
        limit=60,
        scratch_shapes=[pltpu.VMEM((rows, depth), BF16)],
    )
    size = lax.axis_size("z") * lax.axis_size("c")
    onward = [(i, i + 1) for i in range(size - 1)]
    before = lax.ppermute(last, SP, onward)
    after = lax.ppermute(first, SP, [(j, i) for i, j in onward])
    parts = run_feed_forward(pair, tp, normed, before, after, gathered, gate_taps, up_taps)
    summed = across(parts, PEERS).astype(F32).sum(axis=0)
    return (middle.astype(F32) + summed).astype(BF16)


def solution(mesh):
    groups, tp = mesh.shape["grp"], mesh.shape["tp"]
    pair = math.gcd(groups, 2)
    split = Mesh(
        mesh.devices.reshape(groups // pair, pair, mesh.shape["sp"] // 2, 2, tp),
        ("pg", "pr", "z", "c", "tp"),
    )
    placed = (
        P(ROWS, "tp"),
        P(ROWS, "tp"),
        P(ROWS, "tp"),
        P(ROWS, "tp"),
        P(None, "tp", ROWS),
        P(None, "tp"),
        P("tp", None),
        P(ROWS, None),
        P(),
        P(SP, "tp"),
        P(SP, "tp"),
        P(SP, "tp"),
        P(None, "tp"),
        P(None, "tp"),
    )
    return jax.shard_map(
        shards, mesh=split, in_specs=placed, out_specs=P((*ROWS, "tp"), None), check_vma=False
    )
```

```python
import math

import jax
import jax.numpy as jnp
from jax import lax
from jax.experimental import pallas as pl
from jax.experimental.pallas import tpu as pltpu
from jax.sharding import Mesh
from jax.sharding import PartitionSpec as P


HEAD = 128
LANES = 128
SP = ("z", "c")
ROWS = ("pg", "pr", "z", "c")
PEERS = ("pr", "tp")

GROUP_EPS = 1e-05
NORM_EPS = 1e-06


F32 = jnp.float32
BF16 = jnp.bfloat16
VMEM = pl.BlockSpec(memory_space=pltpu.VMEM)
HBM = pl.BlockSpec(memory_space=pltpu.HBM)
BLOCK = 256


def call(body, outs, *args, limit=12, **more):
    spec = {"in_specs": [VMEM] * len(args), "out_specs": jax.tree.map(lambda _: VMEM, outs)}
    return pl.pallas_call(
        body,
        out_shape=outs,
        compiler_params=pltpu.CompilerParams(vmem_limit_bytes=limit << 20),
        **{**spec, **more},
    )(*args)


def shaped(shape, dtype):
    return jax.ShapeDtypeStruct(shape, dtype)


def dot(a, b, dims=((1,), (0,))):
    return lax.dot_general(a, b, (dims, ((), ())), preferred_element_type=F32)


def split_columns(pair, width):
    tiles = width // LANES
    share = -(-tiles // pair)
    step = (tiles - share) // (pair - 1) if pair > 1 else 0
    return share * LANES, step * LANES


def pick_weights(pair, gate_ref, up_ref, down_ref, out_ref, sems):
    cols, step = split_columns(pair, gate_ref.shape[1])
    start = pl.multiple_of(lax.axis_index("pr") * step, LANES)
    blocks = cols // BLOCK
    copies = [
        pltpu.make_async_copy(
            ref.at[:, pl.ds(start + j * BLOCK, BLOCK)],
            out_ref.at[i * blocks + j],
            sems.at[i * blocks + j],
        )
        for i, ref in enumerate((gate_ref, up_ref, down_ref))
        for j in range(blocks)
    ]
    for copy in copies:
        copy.start()
    for copy in copies:
        copy.wait()


def fetch(pairs, sems):
    copies = [pltpu.make_async_copy(src, dst, sems.at[i]) for i, (src, dst) in enumerate(pairs)]
    for copy in copies:
        copy.start()
    return copies


def silu(u):
    return u / (1.0 + jnp.exp(-u))


def local_retention(*refs):
    sources, refs = refs[:6], refs[6:]
    weight_ref, inner_ref, query_ref, gated_ref, keep_ref, send_ref, half_ref, *refs = refs
    held, sems = refs[:6], refs[6]
    half = half_ref.shape[0]
    start = pl.multiple_of(lax.axis_index("c") * half, half)
    copies = fetch(
        [*zip(sources, held), (weight_ref.at[pl.ds(start, half), :], half_ref)], sems
    )
    for copy in copies[:6]:
        copy.wait()
    q_ref, k_ref, v_ref, gate_ref, rate_ref, gain_ref = held
    n, width = q_ref.shape
    heads = width // HEAD
    row = lax.broadcasted_iota(jnp.int32, (n, n), 0)
    col = lax.broadcasted_iota(jnp.int32, (n, n), 1)
    scale = HEAD ** (-0.5)
    first = lax.axis_index("c") == 0
    gated = silu(gate_ref[...].astype(F32))
    for way in range(2):
        gated_ref[way] = gated * gain_ref[way : way + 1, :]
    for h in range(heads):
        cut = slice(h * HEAD, (h + 1) * HEAD)
        q, k, v = q_ref[:, cut], k_ref[:, cut], v_ref[:, cut]
        scores = dot(q, k, ((1,), (1,))) * scale
        states, decays = [], []
        for way in range(2):
            rate = rate_ref[way, h : h + 1, :]
            rate_col = jnp.sum(jnp.where(row == col, rate, 0.0), axis=1, keepdims=True)
            seen = col <= row if way == 0 else col >= row
            seen_by = row <= col if way == 0 else row >= col
            total_col = jnp.sum(jnp.where(seen, rate, 0.0), axis=1, keepdims=True)
            total_row = jnp.sum(jnp.where(seen_by, rate_col, 0.0), axis=0, keepdims=True)
            whole = jnp.sum(rate, axis=1, keepdims=True)
            mask = jnp.where(seen, jnp.exp(jnp.minimum(total_col - total_row, 0.0)), 0.0)
            inner_ref[way, :, cut] = dot((scores * mask).astype(BF16), v)
            query_ref[way, :, cut] = (q.astype(F32) * jnp.exp(total_col)).astype(BF16)
            weight = jnp.exp(whole - total_col) * scale
            states.append(dot((k.astype(F32) * weight).astype(BF16), v, ((0,), (0,))))
            decays.append(jnp.broadcast_to(jnp.exp(whole), (1, HEAD)))
        rows = slice(h * HEAD, (h + 1) * HEAD)
        keep_ref[rows, :] = jnp.where(first, states[0], states[1])
        send_ref[rows, :] = jnp.where(first, states[1], states[0])
        mark = slice(heads * HEAD + h, heads * HEAD + h + 1)
        keep_ref[mark, :] = jnp.where(first, decays[0], decays[1])
        send_ref[mark, :] = jnp.where(first, decays[1], decays[0])
    copies[6].wait()


def pack_states(keep_ref, got_ref, out_ref):
    pieces = out_ref.shape[0]
    heads = keep_ref.shape[0] // HEAD
    rows = HEAD // pieces
    marks = []
    for h in range(heads):
        at = heads * HEAD + h
        a = keep_ref[at : at + 1, :] * got_ref[at : at + 1, :]
        high = a.astype(BF16).astype(F32)
        middle = (a - high).astype(BF16).astype(F32)
        low = a - high - middle
        marks += [high, middle, low]
    used = heads * rows
    marks.append(jnp.zeros((out_ref.shape[1] - used - len(marks), LANES), F32))
    marks = jnp.concatenate(marks, axis=0).astype(BF16)
    for z in range(pieces):
        parts = []
        for h in range(heads):
            at = heads * HEAD + h
            cut = slice(h * HEAD + z * rows, h * HEAD + (z + 1) * rows)
            parts.append(keep_ref[cut, :] * got_ref[at : at + 1, :] + got_ref[cut, :])
        out_ref[z, 0:used, :] = jnp.concatenate(parts, axis=0).astype(BF16)
        out_ref[z, used:, :] = marks


def scan_states(in_ref, out_ref):
    pieces, used, _ = out_ref.shape
    first = lax.axis_index("c") == 0
    half = used // 2
    state = jnp.zeros((used, LANES), F32)
    for t in range(pieces):
        j = jnp.where(first, t, pieces - 1 - t)
        part = in_ref[j].astype(F32)
        out_ref[j] = state.astype(BF16)
        decay = [
            jnp.sum(part[used + 3 * h : used + 3 * h + 3, :], axis=0, keepdims=True)
            for h in range(2)
        ]
        decay = jnp.concatenate([jnp.broadcast_to(d, (half, LANES)) for d in decay], axis=0)
        state = state * decay + part[:used, :]


def spread_states(in_ref, keep_ref, own_ref, send_ref):
    pieces, used, _ = in_ref.shape
    heads = own_ref.shape[0] // HEAD
    rows = used // heads
    for h in range(heads):
        at = heads * HEAD + h
        state = jnp.concatenate(
            [in_ref[z].astype(F32)[h * rows : (h + 1) * rows, :] for z in range(pieces)], axis=0
        )
        cut = slice(h * HEAD, (h + 1) * HEAD)
        own_ref[cut, :] = state.astype(BF16)
        send_ref[cut, :] = (state * keep_ref[at : at + 1, :] + keep_ref[cut, :]).astype(BF16)


def group_norm(values):
    centre = values - jnp.mean(values, axis=1, keepdims=True)
    spread = jnp.mean(centre * centre, axis=1, keepdims=True)
    return centre * lax.rsqrt(spread + GROUP_EPS)


def mix(inner_ref, query_ref, own_ref, got_ref, gated_ref, out_ref):
    heads = inner_ref.shape[2] // HEAD
    first = lax.axis_index("c") == 0
    mixed = []
    for h in range(heads):
        cut = slice(h * HEAD, (h + 1) * HEAD)
        own, got = own_ref[cut, :], got_ref[cut, :]
        combined = 0.0
        for way in range(2):
            state = jnp.where(first, own, got) if way == 0 else jnp.where(first, got, own)
            values = inner_ref[way, :, cut] + dot(query_ref[way, :, cut], state)
            combined = combined + group_norm(values) * gated_ref[way, :, cut]
        mixed.append(combined.astype(BF16))
    mixed = jnp.concatenate(mixed, axis=1)
    for p in range(out_ref.shape[0]):
        out_ref[p] = mixed


def project(pair, tp, *refs):
    mixed_ref, weight_ref, *refs = refs
    near, refs = refs[: tp - 1], refs[tp - 1 :]
    far, refs = refs[: tp - 1], refs[tp - 1 :]
    residuals, refs = refs[:pair], refs[pair:]
    gain_ref, normed_ref, middle_ref, first_ref, last_ref, scratch, table, spans, sems = refs
    me, member, core = lax.axis_index("tp"), lax.axis_index("pr"), lax.axis_index("c")
    n, width = mixed_ref.shape[1:]
    half = width // 2
    low = pl.multiple_of(core * half, half)
    high = pl.multiple_of((1 - core) * half, half)
    pairs = [(weight_ref, table.at[0])]
    for d in range(1, tp):
        pairs.append((near[d - 1], table.at[d, pl.ds(0, half)]))
        pairs.append((far[d - 1], table.at[d, pl.ds(half, half)]))
    pairs += [(residuals[s], spans.at[s]) for s in range(pair)]
    copies = fetch(pairs, sems)
    attended = 0.0
    for d in range(tp):
        parts = []
        for s in range(pair):
            i = lax.rem(member + s, pair) * tp + lax.rem(me - d + tp, tp)
            if d == 0:
                parts.append(mixed_ref[i])
            else:
                parts.append(
                    jnp.concatenate(
                        [mixed_ref[i, :, pl.ds(low, half)], mixed_ref[i, :, pl.ds(high, half)]],
                        axis=1,
                    )
                )
        for copy in copies[max(2 * d - 1, 0) : 2 * d + 1]:
            copy.wait()
        attended = attended + dot(jnp.concatenate(parts, axis=0), table[d])
    for copy in copies[2 * tp - 1 :]:
        copy.wait()
    firsts, lasts = [], []
    for s in range(pair):
        part = attended[s * n : (s + 1) * n, :]
        middle = (spans[s].astype(F32) + part).astype(BF16)
        if s == 0:
            scratch[...] = middle
        values = middle.astype(F32)
        scale = lax.rsqrt(jnp.mean(values * values, axis=1, keepdims=True) + NORM_EPS)
        normed = values * scale * gain_ref[...].astype(F32)
        normed_ref[s * n : (s + 1) * n, :] = normed.astype(BF16)
        firsts.append(normed[0:1, :])
        lasts.append(normed[n - 1 : n, :])
    own = middle_ref.shape[0]
    middle_ref[...] = scratch[pl.ds(pl.multiple_of(me * own, own), own), :]
    fill = [jnp.zeros((first_ref.shape[0] - pair, first_ref.shape[1]), F32)]
    first_ref[...] = jnp.concatenate(firsts + fill, axis=0).astype(BF16)
    last_ref[...] = jnp.concatenate(lasts + fill, axis=0).astype(BF16)


def convolved(pre, pair, taps):
    n = (pre.shape[0] - 16) // pair
    row = lax.broadcasted_iota(jnp.int32, (n, pre.shape[1]), 0)
    spans = []
    for s in range(pair):
        x = pre[s * n : (s + 1) * n, :]
        at = pair * n + s
        before = jnp.where(row == 0, pre[at : at + 1, :], pltpu.roll(x, 1, 0))
        after = jnp.where(row == n - 1, pre[at + 8 : at + 9, :], pltpu.roll(x, n - 1, 0))
        spans.append(taps[0:1] * before + taps[1:2] * x + taps[2:3] * after)
    return jnp.concatenate(spans, axis=0)


def feed_forward(
    pair,
    tp,
    x_ref,
    before_ref,
    after_ref,
    gate_ref,
    up_ref,
    down_ref,
    gt_ref,
    ut_ref,
    out_ref,
    rows_ref,
    acc_ref,
):
    j = pl.program_id(0)
    block = gate_ref.shape[3]
    depth = x_ref.shape[1]
    cols, step = split_columns(pair, gt_ref.shape[1])
    member = lax.axis_index("pr")
    at = pl.multiple_of(member * step + j * block, LANES)
    column = at + lax.broadcasted_iota(jnp.int32, (1, block), 1)
    count = x_ref.shape[0]

    @pl.when(j == 0)
    def _():
        rows_ref[0:count, :] = x_ref[...]
        rows_ref[count:, :] = jnp.concatenate([before_ref[...], after_ref[...]], axis=0)

    def branch(weight, taps):
        pre = dot(rows_ref[...], weight.reshape(depth, block)).astype(BF16).astype(F32)
        return convolved(pre, pair, taps)

    gate = branch(gate_ref[...], gt_ref[:, pl.ds(at, block)].astype(F32))
    taps = jnp.where(column >= member * cols, ut_ref[:, pl.ds(at, block)].astype(F32), 0.0)
    up = branch(up_ref[...], taps)
    hidden = (silu(gate) * up).astype(BF16)
    part = dot(hidden, down_ref[...].reshape(depth, block), ((1,), (1,)))
    last = pl.num_programs(0) - 1

    @pl.when(j == 0)
    def _():
        acc_ref[...] = part

    @pl.when((j > 0) & (j < last))
    def _():
        acc_ref[...] += part

    @pl.when(j == last)
    def _():
        rows = out_ref.shape[1]
        for s in range(pair):
            for q in range(tp):
                cut = slice((s * tp + q) * rows, (s * tp + q + 1) * rows)
                whole = acc_ref[cut, :] + part[cut, :] if cols > block else part[cut, :]
                out_ref[lax.rem(member + s, pair) * tp + q] = whole.astype(BF16)


def run_feed_forward(pair, tp, normed, before, after, gathered, gate_taps, up_taps):
    spans, blocks, height, block = gathered.shape
    depth = spans * height
    steps = blocks // 3
    whole = lambda a: pl.BlockSpec(a.shape, lambda j: (0,) * a.ndim)
    piece = lambda i: pl.BlockSpec(
        (spans, 1, height, block), lambda j, i=i: (0, i * steps + j, 0, 0)
    )
    rows = normed.shape[0]
    out = (pair * tp, rows // (pair * tp), depth)
    return pl.pallas_call(
        lambda *refs: feed_forward(pair, tp, *refs),
        grid=(steps,),
        out_shape=shaped(out, BF16),
        in_specs=[whole(normed), whole(before), whole(after), piece(0), piece(1), piece(2)]
        + [whole(gate_taps), whole(up_taps)],
        out_specs=pl.BlockSpec(out, lambda j: (0, 0, 0)),
        scratch_shapes=[pltpu.VMEM((rows + 16, depth), BF16), pltpu.VMEM((rows, depth), F32)],
        compiler_params=pltpu.CompilerParams(vmem_limit_bytes=56 << 20),
    )(normed, before, after, gathered, gathered, gathered, gate_taps, up_taps)


def across(x, axes):
    return lax.all_to_all(x, axes, 0, 0, tiled=True)


def shards(
    query_rows,
    key_rows,
    value_rows,
    gate_rows,
    log_decay,
    head_gain,
    out_weight,
    residual,
    norm_gain,
    gate_weight,
    up_weight,
    down_weight,
    gate_taps,
    up_taps,
):
    pair, chips, tp = lax.axis_size("pr"), lax.axis_size("z"), lax.axis_size("tp")
    peers = pair * tp
    rows, width = query_rows.shape
    depth = residual.shape[1]
    heads = width // HEAD
    cols, _ = split_columns(pair, gate_weight.shape[1])

    blocks = 3 * cols // BLOCK
    picked = call(
        lambda *refs: pick_weights(pair, *refs),
        shaped((blocks, gate_weight.shape[0], BLOCK), BF16),
        gate_weight,
        up_weight,
        down_weight,
        limit=60,
        in_specs=[HBM] * 3,
        scratch_shapes=[pltpu.SemaphoreType.DMA((blocks,))],
    )
    gathered = lax.all_gather(picked, SP, axis=0, tiled=False)

    marked = shaped((heads * HEAD + 8, HEAD), F32)
    inputs = (query_rows, key_rows, value_rows, gate_rows, log_decay, head_gain)
    inner, query, gated, keep, send, half = call(
        local_retention,
        (
            shaped((2, rows, width), F32),
            shaped((2, rows, width), BF16),
            shaped((2, rows, width), F32),
            marked,
            marked,
            shaped((width // 2, depth), BF16),
        ),
        *inputs,
        out_weight,
        limit=60,
        in_specs=[HBM] * 7,
        scratch_shapes=[pltpu.VMEM(a.shape, a.dtype) for a in inputs]
        + [pltpu.SemaphoreType.DMA((7,))],
    )
    swap = [(0, 1), (1, 0)]
    got = lax.ppermute(send, "c", swap)
    near, far, residuals = [], [], [residual]
    for d in range(1, tp):
        near.append(lax.ppermute(half, "tp", [(i, (i + d) % tp) for i in range(tp)]))
    for a in near:
        far.append(lax.ppermute(a, "c", swap))
    for s in range(1, pair):
        residuals.append(lax.ppermute(residual, "pr", [((i + s) % pair, i) for i in range(pair)]))
    used = heads * HEAD // chips
    message = call(pack_states, shaped((chips, used + 8, HEAD), BF16), keep, got)
    arrived = across(message, "z")
    prefix = call(scan_states, shaped((chips, used, HEAD), BF16), arrived)
    returned = across(prefix, "z")
    state = shaped((heads * HEAD, HEAD), BF16)
    own, other = call(spread_states, (state, state), returned, keep)
    entering = lax.ppermute(other, "c", swap)
    shape = shaped((peers, rows, width), BF16)
    mixed = call(mix, shape, inner, query, own, entering, gated, limit=60)
    edge = shaped((8, depth), BF16)
    normed, middle, first, last = call(
        lambda *refs: project(pair, tp, *refs),
        (shaped((pair * rows, depth), BF16), shaped((rows // tp, depth), BF16), edge, edge),
        across(mixed, PEERS),
        out_weight,
        *near,
        *far,
        *residuals,
        norm_gain.reshape(1, depth),
        limit=60,
        in_specs=[VMEM] + [HBM] * (2 * tp - 1 + pair) + [VMEM],
        scratch_shapes=[
            pltpu.VMEM((rows, depth), BF16),
            pltpu.VMEM((tp, width, depth), BF16),
            pltpu.VMEM((pair, rows, depth), BF16),
            pltpu.SemaphoreType.DMA((2 * tp - 1 + pair,)),
        ],
    )
    size = lax.axis_size("z") * lax.axis_size("c")
    onward = [(i, i + 1) for i in range(size - 1)]
    before = lax.ppermute(last, SP, onward)
    after = lax.ppermute(first, SP, [(j, i) for i, j in onward])
    parts = run_feed_forward(pair, tp, normed, before, after, gathered, gate_taps, up_taps)
    summed = across(parts, PEERS).astype(F32).sum(axis=0)
    return (middle.astype(F32) + summed).astype(BF16)


def solution(mesh):
    groups, tp = mesh.shape["grp"], mesh.shape["tp"]
    pair = math.gcd(groups, 2)
    split = Mesh(
        mesh.devices.reshape(groups // pair, pair, mesh.shape["sp"] // 2, 2, tp),
        ("pg", "pr", "z", "c", "tp"),
    )
    placed = (
        P(ROWS, "tp"),
        P(ROWS, "tp"),
        P(ROWS, "tp"),
        P(ROWS, "tp"),
        P(None, "tp", ROWS),
        P(None, "tp"),
        P("tp", None),
        P(ROWS, None),
        P(),
        P(SP, "tp"),
        P(SP, "tp"),
        P(SP, "tp"),
        P(None, "tp"),
        P(None, "tp"),
    )

    return jax.shard_map(
        shards, mesh=split, in_specs=placed, out_specs=P((*ROWS, "tp"), None), check_vma=False
    )
```

```python
import math

import jax
import jax.numpy as jnp
from jax import lax
from jax.experimental import pallas as pl
from jax.experimental.pallas import tpu as pltpu
from jax.sharding import Mesh
from jax.sharding import PartitionSpec as P


HEAD = 128
LANES = 128
SP = ("z", "c")
ROWS = ("pg", "pr", "z", "c")
PEERS = ("pr", "tp")

GROUP_EPS = 1e-05
NORM_EPS = 1e-06


F32 = jnp.float32
BF16 = jnp.bfloat16
VMEM = pl.BlockSpec(memory_space=pltpu.VMEM)
HBM = pl.BlockSpec(memory_space=pltpu.HBM)
BLOCK = 256


def call(body, outs, *args, limit=12, **more):
    spec = {"in_specs": [VMEM] * len(args), "out_specs": jax.tree.map(lambda _: VMEM, outs)}
    return pl.pallas_call(
        body,
        out_shape=outs,
        compiler_params=pltpu.CompilerParams(vmem_limit_bytes=limit << 20),
        **{**spec, **more},
    )(*args)


def shaped(shape, dtype):
    return jax.ShapeDtypeStruct(shape, dtype)


def near_by(shape, dtype):
    return pltpu.VMEM(shape, dtype)


def dot(a, b, dims=((1,), (0,))):
    return lax.dot_general(a, b, (dims, ((), ())), preferred_element_type=F32)


def split_columns(pair, width):
    tiles = width // LANES
    share = -(-tiles // pair)
    step = (tiles - share) // (pair - 1) if pair > 1 else 0
    return share * LANES, step * LANES


def pick_weights(pair, gate_ref, up_ref, down_ref, out_ref, held, arrived, left):
    cols, step = split_columns(pair, gate_ref.shape[1])
    start = pl.multiple_of(lax.axis_index("pr") * step, LANES)
    blocks = cols // BLOCK
    sources = [
        ref.at[:, pl.ds(start + j * BLOCK, BLOCK)]
        for ref in (gate_ref, up_ref, down_ref)
        for j in range(blocks)
    ]
    copies = fetch([(src, held.at[k]) for k, src in enumerate(sources)], arrived)
    sends = []
    for k, copy in enumerate(copies):
        copy.wait()
        sends.append(pltpu.make_async_copy(held.at[k], out_ref.at[k], left.at[k]))
        sends[-1].start()
    for send in sends:
        send.wait()


def fetch(pairs, sems):
    copies = [pltpu.make_async_copy(src, dst, sems.at[i]) for i, (src, dst) in enumerate(pairs)]
    for copy in copies:
        copy.start()
    return copies


def silu(u):
    return u / (1.0 + jnp.exp(-u))


def local_retention(*refs):
    sources, refs = refs[:6], refs[6:]
    weight_ref, inner_ref, query_ref, gated_ref, keep_ref, send_ref, half_ref, *refs = refs
    held, sems = refs[:6], refs[6]
    half = half_ref.shape[0]
    start = pl.multiple_of(lax.axis_index("c") * half, half)
    copies = fetch(
        [*zip(sources, held), (weight_ref.at[pl.ds(start, half), :], half_ref)], sems
    )
    for copy in copies[:6]:
        copy.wait()
    q_ref, k_ref, v_ref, gate_ref, rate_ref, gain_ref = held
    n, width = q_ref.shape
    heads = width // HEAD
    row = lax.broadcasted_iota(jnp.int32, (n, n), 0)
    col = lax.broadcasted_iota(jnp.int32, (n, n), 1)
    scale = HEAD ** (-0.5)
    first = lax.axis_index("c") == 0
    gated = silu(gate_ref[...].astype(F32))
    for way in range(2):
        gated_ref[way] = gated * gain_ref[way : way + 1, :]
    for h in range(heads):
        cut = slice(h * HEAD, (h + 1) * HEAD)
        q, k, v = q_ref[:, cut], k_ref[:, cut], v_ref[:, cut]
        scores = dot(q, k, ((1,), (1,))) * scale
        states, decays = [], []
        for way in range(2):
            rate = rate_ref[way, h : h + 1, :]
            rate_col = jnp.sum(jnp.where(row == col, rate, 0.0), axis=1, keepdims=True)
            seen = col <= row if way == 0 else col >= row
            seen_by = row <= col if way == 0 else row >= col
            total_col = jnp.sum(jnp.where(seen, rate, 0.0), axis=1, keepdims=True)
            total_row = jnp.sum(jnp.where(seen_by, rate_col, 0.0), axis=0, keepdims=True)
            whole = jnp.sum(rate, axis=1, keepdims=True)
            mask = jnp.where(seen, jnp.exp(jnp.minimum(total_col - total_row, 0.0)), 0.0)
            inner_ref[way, :, cut] = dot((scores * mask).astype(BF16), v)
            query_ref[way, :, cut] = (q.astype(F32) * jnp.exp(total_col)).astype(BF16)
            weight = jnp.exp(whole - total_col) * scale
            states.append(dot((k.astype(F32) * weight).astype(BF16), v, ((0,), (0,))))
            decays.append(jnp.broadcast_to(jnp.exp(whole), (1, HEAD)))
        rows = slice(h * HEAD, (h + 1) * HEAD)
        keep_ref[rows, :] = jnp.where(first, states[0], states[1])
        send_ref[rows, :] = jnp.where(first, states[1], states[0])
        mark = slice(heads * HEAD + h, heads * HEAD + h + 1)
        keep_ref[mark, :] = jnp.where(first, decays[0], decays[1])
        send_ref[mark, :] = jnp.where(first, decays[1], decays[0])
    copies[6].wait()


def pack_states(keep_ref, got_ref, out_ref):
    pieces = out_ref.shape[0]
    heads = keep_ref.shape[0] // HEAD
    rows = HEAD // pieces
    marks = []
    for h in range(heads):
        at = heads * HEAD + h
        a = keep_ref[at : at + 1, :] * got_ref[at : at + 1, :]
        high = a.astype(BF16).astype(F32)
        middle = (a - high).astype(BF16).astype(F32)
        low = a - high - middle
        marks += [high, middle, low]
    used = heads * rows
    marks.append(jnp.zeros((out_ref.shape[1] - used - len(marks), LANES), F32))
    marks = jnp.concatenate(marks, axis=0).astype(BF16)
    for z in range(pieces):
        parts = []
        for h in range(heads):
            at = heads * HEAD + h
            cut = slice(h * HEAD + z * rows, h * HEAD + (z + 1) * rows)
            parts.append(keep_ref[cut, :] * got_ref[at : at + 1, :] + got_ref[cut, :])
        out_ref[z, 0:used, :] = jnp.concatenate(parts, axis=0).astype(BF16)
        out_ref[z, used:, :] = marks


def scan_states(in_ref, out_ref):
    pieces, used, _ = out_ref.shape
    first = lax.axis_index("c") == 0
    half = used // 2
    state = jnp.zeros((used, LANES), F32)
    for t in range(pieces):
        j = jnp.where(first, t, pieces - 1 - t)
        part = in_ref[j].astype(F32)
        out_ref[j] = state.astype(BF16)
        decay = [
            jnp.sum(part[used + 3 * h : used + 3 * h + 3, :], axis=0, keepdims=True)
            for h in range(2)
        ]
        decay = jnp.concatenate([jnp.broadcast_to(d, (half, LANES)) for d in decay], axis=0)
        state = state * decay + part[:used, :]


def spread_states(in_ref, keep_ref, own_ref, send_ref):
    pieces, used, _ = in_ref.shape
    heads = own_ref.shape[0] // HEAD
    rows = used // heads
    for h in range(heads):
        at = heads * HEAD + h
        state = jnp.concatenate(
            [in_ref[z].astype(F32)[h * rows : (h + 1) * rows, :] for z in range(pieces)], axis=0
        )
        cut = slice(h * HEAD, (h + 1) * HEAD)
        own_ref[cut, :] = state.astype(BF16)
        send_ref[cut, :] = (state * keep_ref[at : at + 1, :] + keep_ref[cut, :]).astype(BF16)


def group_norm(values):
    centre = values - jnp.mean(values, axis=1, keepdims=True)
    spread = jnp.mean(centre * centre, axis=1, keepdims=True)
    return centre * lax.rsqrt(spread + GROUP_EPS)


def mix(inner_ref, query_ref, own_ref, got_ref, gated_ref, out_ref):
    heads = inner_ref.shape[2] // HEAD
    first = lax.axis_index("c") == 0
    mixed = []
    for h in range(heads):
        cut = slice(h * HEAD, (h + 1) * HEAD)
        own, got = own_ref[cut, :], got_ref[cut, :]
        combined = 0.0
        for way in range(2):
            state = jnp.where(first, own, got) if way == 0 else jnp.where(first, got, own)
            values = inner_ref[way, :, cut] + dot(query_ref[way, :, cut], state)
            combined = combined + group_norm(values) * gated_ref[way, :, cut]
        mixed.append(combined.astype(BF16))
    mixed = jnp.concatenate(mixed, axis=1)
    for p in range(out_ref.shape[0]):
        out_ref[p] = mixed


def project(pair, tp, *refs):
    mixed_ref, weight_ref, *refs = refs
    near, refs = refs[: tp - 1], refs[tp - 1 :]
    far, refs = refs[: tp - 1], refs[tp - 1 :]
    residuals, refs = refs[:pair], refs[pair:]
    gain_ref, normed_ref, middle_ref, first_ref, last_ref, scratch, table, spans, sems = refs
    me, member, core = lax.axis_index("tp"), lax.axis_index("pr"), lax.axis_index("c")
    n, width = mixed_ref.shape[1:]
    half = width // 2
    low = pl.multiple_of(core * half, half)
    high = pl.multiple_of((1 - core) * half, half)
    pairs = [(weight_ref, table.at[0])]
    for d in range(1, tp):
        pairs.append((near[d - 1], table.at[d, pl.ds(0, half)]))
        pairs.append((far[d - 1], table.at[d, pl.ds(half, half)]))
    pairs += [(residuals[s], spans.at[s]) for s in range(pair)]
    copies = fetch(pairs, sems)
    attended = 0.0
    for d in range(tp):
        parts = []
        for s in range(pair):
            i = lax.rem(member + s, pair) * tp + lax.rem(me - d + tp, tp)
            if d == 0:
                parts.append(mixed_ref[i])
            else:
                parts.append(
                    jnp.concatenate(
                        [mixed_ref[i, :, pl.ds(low, half)], mixed_ref[i, :, pl.ds(high, half)]],
                        axis=1,
                    )
                )
        for copy in copies[max(2 * d - 1, 0) : 2 * d + 1]:
            copy.wait()
        attended = attended + dot(jnp.concatenate(parts, axis=0), table[d])
    for copy in copies[2 * tp - 1 :]:
        copy.wait()
    firsts, lasts = [], []
    for s in range(pair):
        part = attended[s * n : (s + 1) * n, :]
        middle = (spans[s].astype(F32) + part).astype(BF16)
        if s == 0:
            scratch[...] = middle
        values = middle.astype(F32)
        scale = lax.rsqrt(jnp.mean(values * values, axis=1, keepdims=True) + NORM_EPS)
        normed = values * scale * gain_ref[...].astype(F32)
        normed_ref[s * n : (s + 1) * n, :] = normed.astype(BF16)
        firsts.append(normed[0:1, :])
        lasts.append(normed[n - 1 : n, :])
    own = middle_ref.shape[0]
    middle_ref[...] = scratch[pl.ds(pl.multiple_of(me * own, own), own), :]
    fill = [jnp.zeros((first_ref.shape[0] - pair, first_ref.shape[1]), F32)]
    first_ref[...] = jnp.concatenate(firsts + fill, axis=0).astype(BF16)
    last_ref[...] = jnp.concatenate(lasts + fill, axis=0).astype(BF16)


def convolved(pre, pair, taps):
    n = (pre.shape[0] - 16) // pair
    row = lax.broadcasted_iota(jnp.int32, (n, pre.shape[1]), 0)
    spans = []
    for s in range(pair):
        x = pre[s * n : (s + 1) * n, :]
        at = pair * n + s
        before = jnp.where(row == 0, pre[at : at + 1, :], pltpu.roll(x, 1, 0))
        after = jnp.where(row == n - 1, pre[at + 8 : at + 9, :], pltpu.roll(x, n - 1, 0))
        spans.append(taps[0:1] * before + taps[1:2] * x + taps[2:3] * after)
    return jnp.concatenate(spans, axis=0)


def feed_forward(pair, tp, ahead, *refs):
    x_ref, before_ref, after_ref, table_ref, gt_ref, ut_ref, out_ref, *refs = refs
    rows_ref, into, back, x_sem, sems = refs
    _, blocks, _, block = table_ref.shape
    steps = blocks // 3
    count, depth = x_ref.shape
    order = [i * steps + j for j in range(steps) for i in range(2)]
    order += [2 * steps + j for j in range(steps)]
    place = lambda i: pl.ds(i * block, block)
    copies = []
    for k in order:
        i, j = k // steps, k % steps
        target = into.at[j, :, :, place(i)] if i < 2 else back.at[:, :, place(j)]
        copies.append(pltpu.make_async_copy(table_ref.at[:, k], target, sems.at[k]))
    rows_copy = pltpu.make_async_copy(x_ref, rows_ref.at[pl.ds(0, count), :], x_sem)
    rows_copy.start()
    for copy in copies[:ahead]:
        copy.start()
    rows_ref[count:, :] = jnp.concatenate([before_ref[...], after_ref[...]], axis=0)
    cols, step = split_columns(pair, gt_ref.shape[1])
    member = lax.axis_index("pr")

    def arrive(first, last):
        for i in range(first, last):
            copies[i].wait()
            if i + ahead < len(copies):
                copies[i + ahead].start()

    rows_copy.wait()
    hidden = []
    for j in range(steps):
        at = pl.multiple_of(member * step + j * block, LANES)
        column = at + lax.broadcasted_iota(jnp.int32, (1, block), 1)
        up_taps = jnp.where(column >= member * cols, ut_ref[:, pl.ds(at, block)].astype(F32), 0.0)
        taps = jnp.concatenate([gt_ref[:, pl.ds(at, block)].astype(F32), up_taps], axis=1)
        arrive(2 * j, 2 * j + 2)
        pre = dot(rows_ref[...], into[j].reshape(depth, 2 * block)).astype(BF16).astype(F32)
        both = convolved(pre, pair, taps)
        hidden.append((silu(both[:, :block]) * both[:, block:]).astype(BF16))
    arrive(2 * steps, 3 * steps)
    rows = out_ref.shape[1]
    whole = back[...].reshape(depth, steps * block)
    part = dot(jnp.concatenate(hidden, axis=1), whole, ((1,), (1,)))
    for s in range(pair):
        for q in range(tp):
            cut = slice((s * tp + q) * rows, (s * tp + q + 1) * rows)
            out_ref[lax.rem(member + s, pair) * tp + q] = part[cut, :].astype(BF16)


def run_feed_forward(pair, tp, normed, before, after, gathered, gate_taps, up_taps, ahead=6):
    spans, blocks, height, block = gathered.shape
    steps = blocks // 3
    rows, depth = normed.shape
    return call(
        lambda *refs: feed_forward(pair, tp, ahead, *refs),
        near_by((pair * tp, rows // (pair * tp), depth), BF16),
        normed,
        before,
        after,
        gathered,
        gate_taps,
        up_taps,
        limit=55,
        in_specs=[HBM, VMEM, VMEM, HBM, VMEM, VMEM],
        scratch_shapes=[
            pltpu.VMEM((rows + 16, depth), BF16),
            pltpu.VMEM((steps, spans, height, 2 * block), BF16),
            pltpu.VMEM((spans, height, steps * block), BF16),
            pltpu.SemaphoreType.DMA,
            pltpu.SemaphoreType.DMA((blocks,)),
        ],
    )


def across(x, axes):
    return lax.all_to_all(x, axes, 0, 0, tiled=True)


def shards(
    query_rows,
    key_rows,
    value_rows,
    gate_rows,
    log_decay,
    head_gain,
    out_weight,
    residual,
    norm_gain,
    gate_weight,
    up_weight,
    down_weight,
    gate_taps,
    up_taps,
):
    pair, chips, tp = lax.axis_size("pr"), lax.axis_size("z"), lax.axis_size("tp")
    peers = pair * tp
    rows, width = query_rows.shape
    depth = residual.shape[1]
    heads = width // HEAD
    cols, _ = split_columns(pair, gate_weight.shape[1])

    blocks = 3 * cols // BLOCK
    picked = call(
        lambda *refs: pick_weights(pair, *refs),
        shaped((blocks, gate_weight.shape[0], BLOCK), BF16),
        gate_weight,
        up_weight,
        down_weight,
        limit=60,
        in_specs=[HBM] * 3,
        out_specs=HBM,
        scratch_shapes=[pltpu.VMEM((blocks, gate_weight.shape[0], BLOCK), BF16)]
        + [pltpu.SemaphoreType.DMA((blocks,))] * 2,
    )
    gathered = lax.all_gather(picked, SP, axis=0, tiled=False)

    marked = near_by((heads * HEAD + 8, HEAD), F32)
    inputs = (query_rows, key_rows, value_rows, gate_rows, log_decay, head_gain)
    inner, query, gated, keep, send, half = call(
        local_retention,
        (
            near_by((2, rows, width), F32),
            near_by((2, rows, width), BF16),
            near_by((2, rows, width), F32),
            marked,
            marked,
            shaped((width // 2, depth), BF16),
        ),
        *inputs,
        out_weight,
        limit=60,
        in_specs=[HBM] * 7,
        scratch_shapes=[pltpu.VMEM(a.shape, a.dtype) for a in inputs]
        + [pltpu.SemaphoreType.DMA((7,))],
    )
    swap = [(0, 1), (1, 0)]
    got = lax.ppermute(send, "c", swap)
    near, far, residuals = [], [], [residual]
    for d in range(1, tp):
        near.append(lax.ppermute(half, "tp", [(i, (i + d) % tp) for i in range(tp)]))
    for a in near:
        far.append(lax.ppermute(a, "c", swap))
    for s in range(1, pair):
        residuals.append(lax.ppermute(residual, "pr", [((i + s) % pair, i) for i in range(pair)]))
    used = heads * HEAD // chips
    message = call(pack_states, near_by((chips, used + 8, HEAD), BF16), keep, got)
    arrived = across(message, "z")
    prefix = call(scan_states, near_by((chips, used, HEAD), BF16), arrived)
    returned = across(prefix, "z")
    state = near_by((heads * HEAD, HEAD), BF16)
    own, other = call(spread_states, (state, state), returned, keep)
    entering = lax.ppermute(other, "c", swap)
    shape = near_by((peers, rows, width), BF16)
    mixed = call(mix, shape, inner, query, own, entering, gated)
    edge = near_by((8, depth), BF16)
    normed, middle, first, last = call(
        lambda *refs: project(pair, tp, *refs),
        (near_by((pair * rows, depth), BF16), near_by((rows // tp, depth), BF16), edge, edge),
        across(mixed, PEERS),
        out_weight,
        *near,
        *far,
        *residuals,
        norm_gain.reshape(1, depth),
        limit=60,
        in_specs=[VMEM] + [HBM] * (2 * tp - 1 + pair) + [VMEM],
        scratch_shapes=[
            pltpu.VMEM((rows, depth), BF16),
            pltpu.VMEM((tp, width, depth), BF16),
            pltpu.VMEM((pair, rows, depth), BF16),
            pltpu.SemaphoreType.DMA((2 * tp - 1 + pair,)),
        ],
    )
    size = lax.axis_size("z") * lax.axis_size("c")
    onward = [(i, i + 1) for i in range(size - 1)]
    before = lax.ppermute(last, SP, onward)
    after = lax.ppermute(first, SP, [(j, i) for i, j in onward])
    parts = run_feed_forward(pair, tp, normed, before, after, gathered, gate_taps, up_taps)
    summed = across(parts, PEERS).astype(F32).sum(axis=0)
    return (middle.astype(F32) + summed).astype(BF16)


def solution(mesh):
    groups, tp = mesh.shape["grp"], mesh.shape["tp"]
    pair = math.gcd(groups, 2)
    split = Mesh(
        mesh.devices.reshape(groups // pair, pair, mesh.shape["sp"] // 2, 2, tp),
        ("pg", "pr", "z", "c", "tp"),
    )
    placed = (
        P(ROWS, "tp"),
        P(ROWS, "tp"),
        P(ROWS, "tp"),
        P(ROWS, "tp"),
        P(None, "tp", ROWS),
        P(None, "tp"),
        P("tp", None),
        P(ROWS, None),
        P(),
        P(SP, "tp"),
        P(SP, "tp"),
        P(SP, "tp"),
        P(None, "tp"),
        P(None, "tp"),
    )

    return jax.shard_map(
        shards, mesh=split, in_specs=placed, out_specs=P((*ROWS, "tp"), None), check_vma=False
    )
```

```python
import math

import jax
import jax.numpy as jnp
from jax import lax
from jax.experimental import pallas as pl
from jax.experimental.pallas import tpu as pltpu
from jax.sharding import Mesh
from jax.sharding import PartitionSpec as P


HEAD = 128
LANES = 128
SP = ("z", "c")
ROWS = ("pg", "pr", "z", "c")
PEERS = ("pr", "tp")

GROUP_EPS = 1e-05
NORM_EPS = 1e-06


F32 = jnp.float32
BF16 = jnp.bfloat16
VMEM = pl.BlockSpec(memory_space=pltpu.VMEM)
HBM = pl.BlockSpec(memory_space=pltpu.HBM)
BLOCK = 256


def call(body, outs, *args, limit=12, **more):
    spec = {"in_specs": [VMEM] * len(args), "out_specs": jax.tree.map(lambda _: VMEM, outs)}
    return pl.pallas_call(
        body,
        out_shape=outs,
        compiler_params=pltpu.CompilerParams(vmem_limit_bytes=limit << 20),
        **{**spec, **more},
    )(*args)


def shaped(shape, dtype):
    return jax.ShapeDtypeStruct(shape, dtype)


def near_by(shape, dtype):
    return pltpu.VMEM(shape, dtype)


def dot(a, b, dims=((1,), (0,))):
    return lax.dot_general(a, b, (dims, ((), ())), preferred_element_type=F32)


def split_columns(pair, width):
    tiles = width // LANES
    share = -(-tiles // pair)
    step = (tiles - share) // (pair - 1) if pair > 1 else 0
    return share * LANES, step * LANES


def pick_weights(pair, gate_ref, up_ref, down_ref, out_ref, held, arrived, left):
    cols, step = split_columns(pair, gate_ref.shape[1])
    start = pl.multiple_of(lax.axis_index("pr") * step, LANES)
    blocks = cols // BLOCK
    sources = [
        ref.at[:, pl.ds(start + j * BLOCK, BLOCK)]
        for ref in (gate_ref, up_ref, down_ref)
        for j in range(blocks)
    ]
    copies = fetch([(src, held.at[k]) for k, src in enumerate(sources)], arrived)
    sends = []
    for k, copy in enumerate(copies):
        copy.wait()
        sends.append(pltpu.make_async_copy(held.at[k], out_ref.at[k], left.at[k]))
        sends[-1].start()
    for send in sends:
        send.wait()


def fetch(pairs, sems):
    copies = [pltpu.make_async_copy(src, dst, sems.at[i]) for i, (src, dst) in enumerate(pairs)]
    for copy in copies:
        copy.start()
    return copies


def silu(u):
    return u / (1.0 + jnp.exp(-u))


def local_retention(*refs):
    sources, refs = refs[:6], refs[6:]
    weight_ref, inner_ref, query_ref, gated_ref, keep_ref, send_ref, half_ref, *refs = refs
    held, sems = refs[:6], refs[6]
    half = half_ref.shape[0]
    start = pl.multiple_of(lax.axis_index("c") * half, half)
    copies = fetch(
        [*zip(sources, held), (weight_ref.at[pl.ds(start, half), :], half_ref)], sems
    )
    for copy in copies[:6]:
        copy.wait()
    q_ref, k_ref, v_ref, gate_ref, rate_ref, gain_ref = held
    n, width = q_ref.shape
    heads = width // HEAD
    row = lax.broadcasted_iota(jnp.int32, (n, n), 0)
    col = lax.broadcasted_iota(jnp.int32, (n, n), 1)
    scale = HEAD ** (-0.5)
    first = lax.axis_index("c") == 0
    gated = silu(gate_ref[...].astype(F32))
    for way in range(2):
        gated_ref[way] = gated * gain_ref[way : way + 1, :]
    for h in range(heads):
        cut = slice(h * HEAD, (h + 1) * HEAD)
        q, k, v = q_ref[:, cut], k_ref[:, cut], v_ref[:, cut]
        scores = dot(q, k, ((1,), (1,))) * scale
        states, decays = [], []
        for way in range(2):
            rate = rate_ref[way, h : h + 1, :]
            rate_col = jnp.sum(jnp.where(row == col, rate, 0.0), axis=1, keepdims=True)
            seen = col <= row if way == 0 else col >= row
            seen_by = row <= col if way == 0 else row >= col
            total_col = jnp.sum(jnp.where(seen, rate, 0.0), axis=1, keepdims=True)
            total_row = jnp.sum(jnp.where(seen_by, rate_col, 0.0), axis=0, keepdims=True)
            whole = jnp.sum(rate, axis=1, keepdims=True)
            mask = jnp.where(seen, jnp.exp(jnp.minimum(total_col - total_row, 0.0)), 0.0)
            inner_ref[way, :, cut] = dot((scores * mask).astype(BF16), v)
            query_ref[way, :, cut] = (q.astype(F32) * jnp.exp(total_col)).astype(BF16)
            weight = jnp.exp(whole - total_col) * scale
            states.append(dot((k.astype(F32) * weight).astype(BF16), v, ((0,), (0,))))
            decays.append(jnp.broadcast_to(jnp.exp(whole), (1, HEAD)))
        rows = slice(h * HEAD, (h + 1) * HEAD)
        keep_ref[rows, :] = jnp.where(first, states[0], states[1])
        send_ref[rows, :] = jnp.where(first, states[1], states[0])
        mark = slice(heads * HEAD + h, heads * HEAD + h + 1)
        keep_ref[mark, :] = jnp.where(first, decays[0], decays[1])
        send_ref[mark, :] = jnp.where(first, decays[1], decays[0])
    copies[6].wait()


def pack_states(keep_ref, got_ref, out_ref):
    pieces = out_ref.shape[0]
    heads = keep_ref.shape[0] // HEAD
    rows = HEAD // pieces
    marks = []
    for h in range(heads):
        at = heads * HEAD + h
        a = keep_ref[at : at + 1, :] * got_ref[at : at + 1, :]
        high = a.astype(BF16).astype(F32)
        middle = (a - high).astype(BF16).astype(F32)
        low = a - high - middle
        marks += [high, middle, low]
    used = heads * rows
    marks.append(jnp.zeros((out_ref.shape[1] - used - len(marks), LANES), F32))
    marks = jnp.concatenate(marks, axis=0).astype(BF16)
    for z in range(pieces):
        parts = []
        for h in range(heads):
            at = heads * HEAD + h
            cut = slice(h * HEAD + z * rows, h * HEAD + (z + 1) * rows)
            parts.append(keep_ref[cut, :] * got_ref[at : at + 1, :] + got_ref[cut, :])
        out_ref[z, 0:used, :] = jnp.concatenate(parts, axis=0).astype(BF16)
        out_ref[z, used:, :] = marks


def scan_states(in_ref, out_ref):
    pieces, used, _ = out_ref.shape
    first = lax.axis_index("c") == 0
    half = used // 2
    state = jnp.zeros((used, LANES), F32)
    for t in range(pieces):
        j = jnp.where(first, t, pieces - 1 - t)
        part = in_ref[j].astype(F32)
        out_ref[j] = state.astype(BF16)
        decay = [
            jnp.sum(part[used + 3 * h : used + 3 * h + 3, :], axis=0, keepdims=True)
            for h in range(2)
        ]
        decay = jnp.concatenate([jnp.broadcast_to(d, (half, LANES)) for d in decay], axis=0)
        state = state * decay + part[:used, :]


def spread_states(in_ref, keep_ref, own_ref, send_ref):
    pieces, used, _ = in_ref.shape
    heads = own_ref.shape[0] // HEAD
    rows = used // heads
    for h in range(heads):
        at = heads * HEAD + h
        state = jnp.concatenate(
            [in_ref[z].astype(F32)[h * rows : (h + 1) * rows, :] for z in range(pieces)], axis=0
        )
        cut = slice(h * HEAD, (h + 1) * HEAD)
        own_ref[cut, :] = state.astype(BF16)
        send_ref[cut, :] = (state * keep_ref[at : at + 1, :] + keep_ref[cut, :]).astype(BF16)


def group_norm(values):
    centre = values - jnp.mean(values, axis=1, keepdims=True)
    spread = jnp.mean(centre * centre, axis=1, keepdims=True)
    return centre * lax.rsqrt(spread + GROUP_EPS)


def mix(inner_ref, query_ref, own_ref, got_ref, gated_ref, out_ref):
    heads = inner_ref.shape[2] // HEAD
    first = lax.axis_index("c") == 0
    mixed = []
    for h in range(heads):
        cut = slice(h * HEAD, (h + 1) * HEAD)
        own, got = own_ref[cut, :], got_ref[cut, :]
        combined = 0.0
        for way in range(2):
            state = jnp.where(first, own, got) if way == 0 else jnp.where(first, got, own)
            values = inner_ref[way, :, cut] + dot(query_ref[way, :, cut], state)
            combined = combined + group_norm(values) * gated_ref[way, :, cut]
        mixed.append(combined.astype(BF16))
    mixed = jnp.concatenate(mixed, axis=1)
    for p in range(out_ref.shape[0]):
        out_ref[p] = mixed


def project(pair, tp, *refs):
    mixed_ref, weight_ref, *refs = refs
    near, refs = refs[: tp - 1], refs[tp - 1 :]
    far, refs = refs[: tp - 1], refs[tp - 1 :]
    residuals, refs = refs[:pair], refs[pair:]
    gain_ref, normed_ref, middle_ref, first_ref, last_ref, scratch, table, spans, sems = refs
    me, member, core = lax.axis_index("tp"), lax.axis_index("pr"), lax.axis_index("c")
    n, width = mixed_ref.shape[1:]
    half = width // 2
    low = pl.multiple_of(core * half, half)
    high = pl.multiple_of((1 - core) * half, half)
    pairs = [(weight_ref, table.at[0])]
    for d in range(1, tp):
        pairs.append((near[d - 1], table.at[d, pl.ds(0, half)]))
        pairs.append((far[d - 1], table.at[d, pl.ds(half, half)]))
    pairs += [(residuals[s], spans.at[s]) for s in range(pair)]
    copies = fetch(pairs, sems)
    attended = 0.0
    for d in range(tp):
        parts = []
        for s in range(pair):
            i = lax.rem(member + s, pair) * tp + lax.rem(me - d + tp, tp)
            if d == 0:
                parts.append(mixed_ref[i])
            else:
                parts.append(
                    jnp.concatenate(
                        [mixed_ref[i, :, pl.ds(low, half)], mixed_ref[i, :, pl.ds(high, half)]],
                        axis=1,
                    )
                )
        for copy in copies[max(2 * d - 1, 0) : 2 * d + 1]:
            copy.wait()
        attended = attended + dot(jnp.concatenate(parts, axis=0), table[d])
    for copy in copies[2 * tp - 1 :]:
        copy.wait()
    firsts, lasts = [], []
    for s in range(pair):
        part = attended[s * n : (s + 1) * n, :]
        middle = (spans[s].astype(F32) + part).astype(BF16)
        if s == 0:
            scratch[...] = middle
        values = middle.astype(F32)
        scale = lax.rsqrt(jnp.mean(values * values, axis=1, keepdims=True) + NORM_EPS)
        normed = values * scale * gain_ref[...].astype(F32)
        normed_ref[s * n : (s + 1) * n, :] = normed.astype(BF16)
        firsts.append(normed[0:1, :])
        lasts.append(normed[n - 1 : n, :])
    own = middle_ref.shape[0]
    middle_ref[...] = scratch[pl.ds(pl.multiple_of(me * own, own), own), :]
    fill = [jnp.zeros((first_ref.shape[0] - pair, first_ref.shape[1]), F32)]
    first_ref[...] = jnp.concatenate(firsts + fill, axis=0).astype(BF16)
    last_ref[...] = jnp.concatenate(lasts + fill, axis=0).astype(BF16)


def convolved(pre, pair, taps):
    n = (pre.shape[0] - 16) // pair
    row = lax.broadcasted_iota(jnp.int32, (n, pre.shape[1]), 0)
    spans = []
    for s in range(pair):
        x = pre[s * n : (s + 1) * n, :]
        at = pair * n + s
        before = jnp.where(row == 0, pre[at : at + 1, :], pltpu.roll(x, 1, 0))
        after = jnp.where(row == n - 1, pre[at + 8 : at + 9, :], pltpu.roll(x, n - 1, 0))
        spans.append(taps[0:1] * before + taps[1:2] * x + taps[2:3] * after)
    return jnp.concatenate(spans, axis=0)


def feed_forward(pair, tp, ahead, *refs):
    sources, (table_ref, out_ref), refs = refs[:5], refs[5:7], refs[7:]
    (before_ref, after_ref, gt_ref, ut_ref, rows_ref, into, back), sems = refs[:7], refs[7:]
    _, blocks, _, block = table_ref.shape
    steps = blocks // 3
    count, depth = sources[0].shape
    small = fetch(
        [
            *zip(sources[1:], (before_ref, after_ref, gt_ref, ut_ref)),
            (sources[0], rows_ref.at[pl.ds(0, count), :]),
        ],
        sems[0],
    )
    order = [i * steps + j for j in range(steps) for i in range(2)]
    order += [2 * steps + j for j in range(steps)]
    place = lambda i: pl.ds(i * block, block)
    copies = []
    for k in order:
        i, j = k // steps, k % steps
        target = into.at[j, :, :, place(i)] if i < 2 else back.at[:, :, place(j)]
        copies.append(pltpu.make_async_copy(table_ref.at[:, k], target, sems[1].at[k]))
    for copy in copies[:ahead]:
        copy.start()
    for copy in small:
        copy.wait()
    rows_ref[count:, :] = jnp.concatenate([before_ref[...], after_ref[...]], axis=0)
    cols, step = split_columns(pair, gt_ref.shape[1])
    member = lax.axis_index("pr")

    def arrive(first, last):
        for i in range(first, last):
            copies[i].wait()
            if i + ahead < len(copies):
                copies[i + ahead].start()

    hidden = []
    for j in range(steps):
        at = pl.multiple_of(member * step + j * block, LANES)
        column = at + lax.broadcasted_iota(jnp.int32, (1, block), 1)
        up_taps = jnp.where(column >= member * cols, ut_ref[:, pl.ds(at, block)].astype(F32), 0.0)
        taps = jnp.concatenate([gt_ref[:, pl.ds(at, block)].astype(F32), up_taps], axis=1)
        arrive(2 * j, 2 * j + 2)
        pre = dot(rows_ref[...], into[j].reshape(depth, 2 * block)).astype(BF16).astype(F32)
        both = convolved(pre, pair, taps)
        hidden.append((silu(both[:, :block]) * both[:, block:]).astype(BF16))
    arrive(2 * steps, 3 * steps)
    rows = out_ref.shape[1]
    whole = back[...].reshape(depth, steps * block)
    part = dot(jnp.concatenate(hidden, axis=1), whole, ((1,), (1,)))
    for s in range(pair):
        for q in range(tp):
            cut = slice((s * tp + q) * rows, (s * tp + q + 1) * rows)
            out_ref[lax.rem(member + s, pair) * tp + q] = part[cut, :].astype(BF16)


def run_feed_forward(pair, tp, normed, before, after, gathered, gate_taps, up_taps, ahead=6):
    spans, blocks, height, block = gathered.shape
    steps = blocks // 3
    rows, depth = normed.shape
    sources = (normed, before, after, gate_taps, up_taps)
    return call(
        lambda *refs: feed_forward(pair, tp, ahead, *refs),
        near_by((pair * tp, rows // (pair * tp), depth), BF16),
        *sources,
        gathered,
        limit=55,
        in_specs=[HBM] * 6,
        scratch_shapes=[pltpu.VMEM(a.shape, a.dtype) for a in sources[1:]]
        + [
            pltpu.VMEM((rows + 16, depth), BF16),
            pltpu.VMEM((steps, spans, height, 2 * block), BF16),
            pltpu.VMEM((spans, height, steps * block), BF16),
            pltpu.SemaphoreType.DMA((5,)),
            pltpu.SemaphoreType.DMA((blocks,)),
        ],
    )


def across(x, axes):
    return lax.all_to_all(x, axes, 0, 0, tiled=True)


def shards(
    query_rows,
    key_rows,
    value_rows,
    gate_rows,
    log_decay,
    head_gain,
    out_weight,
    residual,
    norm_gain,
    gate_weight,
    up_weight,
    down_weight,
    gate_taps,
    up_taps,
):
    pair, chips, tp = lax.axis_size("pr"), lax.axis_size("z"), lax.axis_size("tp")
    peers = pair * tp
    rows, width = query_rows.shape
    depth = residual.shape[1]
    heads = width // HEAD
    cols, _ = split_columns(pair, gate_weight.shape[1])

    blocks = 3 * cols // BLOCK
    picked = call(
        lambda *refs: pick_weights(pair, *refs),
        shaped((blocks, gate_weight.shape[0], BLOCK), BF16),
        gate_weight,
        up_weight,
        down_weight,
        limit=60,
        in_specs=[HBM] * 3,
        out_specs=HBM,
        scratch_shapes=[pltpu.VMEM((blocks, gate_weight.shape[0], BLOCK), BF16)]
        + [pltpu.SemaphoreType.DMA((blocks,))] * 2,
    )
    gathered = lax.all_gather(picked, SP, axis=0, tiled=False)

    marked = near_by((heads * HEAD + 8, HEAD), F32)
    inputs = (query_rows, key_rows, value_rows, gate_rows, log_decay, head_gain)
    inner, query, gated, keep, send, half = call(
        local_retention,
        (
            near_by((2, rows, width), F32),
            near_by((2, rows, width), BF16),
            near_by((2, rows, width), F32),
            marked,
            marked,
            shaped((width // 2, depth), BF16),
        ),
        *inputs,
        out_weight,
        limit=60,
        in_specs=[HBM] * 7,
        scratch_shapes=[pltpu.VMEM(a.shape, a.dtype) for a in inputs]
        + [pltpu.SemaphoreType.DMA((7,))],
    )
    swap = [(0, 1), (1, 0)]
    got = lax.ppermute(send, "c", swap)
    near, far, residuals = [], [], [residual]
    for d in range(1, tp):
        near.append(lax.ppermute(half, "tp", [(i, (i + d) % tp) for i in range(tp)]))
    for a in near:
        far.append(lax.ppermute(a, "c", swap))
    for s in range(1, pair):
        residuals.append(lax.ppermute(residual, "pr", [((i + s) % pair, i) for i in range(pair)]))
    used = heads * HEAD // chips
    message = call(pack_states, near_by((chips, used + 8, HEAD), BF16), keep, got)
    arrived = across(message, "z")
    prefix = call(scan_states, near_by((chips, used, HEAD), BF16), arrived)
    returned = across(prefix, "z")
    state = near_by((heads * HEAD, HEAD), BF16)
    own, other = call(spread_states, (state, state), returned, keep)
    entering = lax.ppermute(other, "c", swap)
    shape = near_by((peers, rows, width), BF16)
    mixed = call(mix, shape, inner, query, own, entering, gated)
    edge = near_by((8, depth), BF16)
    normed, middle, first, last = call(
        lambda *refs: project(pair, tp, *refs),
        (near_by((pair * rows, depth), BF16), near_by((rows // tp, depth), BF16), edge, edge),
        across(mixed, PEERS),
        out_weight,
        *near,
        *far,
        *residuals,
        norm_gain.reshape(1, depth),
        limit=60,
        in_specs=[VMEM] + [HBM] * (2 * tp - 1 + pair) + [VMEM],
        scratch_shapes=[
            pltpu.VMEM((rows, depth), BF16),
            pltpu.VMEM((tp, width, depth), BF16),
            pltpu.VMEM((pair, rows, depth), BF16),
            pltpu.SemaphoreType.DMA((2 * tp - 1 + pair,)),
        ],
    )
    size = lax.axis_size("z") * lax.axis_size("c")
    onward = [(i, i + 1) for i in range(size - 1)]
    before = lax.ppermute(last, SP, onward)
    after = lax.ppermute(first, SP, [(j, i) for i, j in onward])
    parts = run_feed_forward(pair, tp, normed, before, after, gathered, gate_taps, up_taps)
    summed = across(parts, PEERS).astype(F32).sum(axis=0)
    return (middle.astype(F32) + summed).astype(BF16)


def solution(mesh):
    groups, tp = mesh.shape["grp"], mesh.shape["tp"]
    pair = math.gcd(groups, 2)
    split = Mesh(
        mesh.devices.reshape(groups // pair, pair, mesh.shape["sp"] // 2, 2, tp),
        ("pg", "pr", "z", "c", "tp"),
    )
    placed = (
        P(ROWS, "tp"),
        P(ROWS, "tp"),
        P(ROWS, "tp"),
        P(ROWS, "tp"),
        P(None, "tp", ROWS),
        P(None, "tp"),
        P("tp", None),
        P(ROWS, None),
        P(),
        P(SP, "tp"),
        P(SP, "tp"),
        P(SP, "tp"),
        P(None, "tp"),
        P(None, "tp"),
    )

    return jax.shard_map(
        shards, mesh=split, in_specs=placed, out_specs=P((*ROWS, "tp"), None), check_vma=False
    )
```

```python
import math

import jax
import jax.numpy as jnp
from jax import lax
from jax.experimental import pallas as pl
from jax.experimental.pallas import tpu as pltpu
from jax.sharding import Mesh
from jax.sharding import PartitionSpec as P


HEAD = 128
LANES = 128
SP = ("z", "c")
ROWS = ("pg", "pr", "z", "c")
PEERS = ("pr", "tp")

GROUP_EPS = 1e-05
NORM_EPS = 1e-06


F32 = jnp.float32
BF16 = jnp.bfloat16
VMEM = pl.BlockSpec(memory_space=pltpu.VMEM)
HBM = pl.BlockSpec(memory_space=pltpu.HBM)
BLOCK = 256


def call(body, outs, *args, limit=12, **more):
    spec = {"in_specs": [VMEM] * len(args), "out_specs": jax.tree.map(lambda _: VMEM, outs)}
    return pl.pallas_call(
        body,
        out_shape=outs,
        compiler_params=pltpu.CompilerParams(vmem_limit_bytes=limit << 20),
        **{**spec, **more},
    )(*args)


def shaped(shape, dtype):
    return jax.ShapeDtypeStruct(shape, dtype)


def near_by(shape, dtype):
    return pltpu.VMEM(shape, dtype)


def dot(a, b, dims=((1,), (0,))):
    return lax.dot_general(a, b, (dims, ((), ())), preferred_element_type=F32)


def split_columns(pair, width):
    tiles = width // LANES
    share = -(-tiles // pair)
    step = (tiles - share) // (pair - 1) if pair > 1 else 0
    return share * LANES, step * LANES


def pick_weights(pair, gate_ref, up_ref, down_ref, out_ref, held, arrived, left):
    cols, step = split_columns(pair, gate_ref.shape[1])
    start = pl.multiple_of(lax.axis_index("pr") * step, LANES)
    blocks = cols // BLOCK
    sources = [
        ref.at[:, pl.ds(start + j * BLOCK, BLOCK)]
        for ref in (gate_ref, up_ref, down_ref)
        for j in range(blocks)
    ]
    copies = fetch([(src, held.at[k]) for k, src in enumerate(sources)], arrived)
    sends = []
    for k, copy in enumerate(copies):
        copy.wait()
        sends.append(pltpu.make_async_copy(held.at[k], out_ref.at[k], left.at[k]))
        sends[-1].start()
    for send in sends:
        send.wait()


def fetch(pairs, sems):
    copies = [pltpu.make_async_copy(src, dst, sems.at[i]) for i, (src, dst) in enumerate(pairs)]
    for copy in copies:
        copy.start()
    return copies


def silu(u):
    return u / (1.0 + jnp.exp(-u))


def local_retention(*refs):
    sources, refs = refs[:6], refs[6:]
    weight_ref, inner_ref, query_ref, gated_ref, keep_ref, send_ref, half_ref, *refs = refs
    held, sems = refs[:6], refs[6]
    half = half_ref.shape[0]
    start = pl.multiple_of(lax.axis_index("c") * half, half)
    copies = fetch(
        [*zip(sources, held), (weight_ref.at[pl.ds(start, half), :], half_ref)], sems
    )
    for copy in copies[:6]:
        copy.wait()
    q_ref, k_ref, v_ref, gate_ref, rate_ref, gain_ref = held
    n, width = q_ref.shape
    heads = width // HEAD
    row = lax.broadcasted_iota(jnp.int32, (n, n), 0)
    col = lax.broadcasted_iota(jnp.int32, (n, n), 1)
    scale = HEAD ** (-0.5)
    first = lax.axis_index("c") == 0
    gated = silu(gate_ref[...].astype(F32))
    for way in range(2):
        gated_ref[way] = gated * gain_ref[way : way + 1, :]
    for h in range(heads):
        cut = slice(h * HEAD, (h + 1) * HEAD)
        q, k, v = q_ref[:, cut], k_ref[:, cut], v_ref[:, cut]
        scores = dot(q, k, ((1,), (1,))) * scale
        states, decays = [], []
        for way in range(2):
            rate = rate_ref[way, h : h + 1, :]
            rate_col = jnp.sum(jnp.where(row == col, rate, 0.0), axis=1, keepdims=True)
            seen = col <= row if way == 0 else col >= row
            seen_by = row <= col if way == 0 else row >= col
            total_col = jnp.sum(jnp.where(seen, rate, 0.0), axis=1, keepdims=True)
            total_row = jnp.sum(jnp.where(seen_by, rate_col, 0.0), axis=0, keepdims=True)
            whole = jnp.sum(rate, axis=1, keepdims=True)
            mask = jnp.where(seen, jnp.exp(jnp.minimum(total_col - total_row, 0.0)), 0.0)
            inner_ref[way, :, cut] = dot((scores * mask).astype(BF16), v)
            query_ref[way, :, cut] = (q.astype(F32) * jnp.exp(total_col)).astype(BF16)
            weight = jnp.exp(whole - total_col) * scale
            states.append(dot((k.astype(F32) * weight).astype(BF16), v, ((0,), (0,))))
            decays.append(jnp.broadcast_to(jnp.exp(whole), (1, HEAD)))
        rows = slice(h * HEAD, (h + 1) * HEAD)
        keep_ref[rows, :] = jnp.where(first, states[0], states[1])
        send_ref[rows, :] = jnp.where(first, states[1], states[0])
        mark = slice(heads * HEAD + h, heads * HEAD + h + 1)
        keep_ref[mark, :] = jnp.where(first, decays[0], decays[1])
        send_ref[mark, :] = jnp.where(first, decays[1], decays[0])
    copies[6].wait()


def pack_states(keep_ref, got_ref, out_ref):
    pieces = out_ref.shape[0]
    heads = keep_ref.shape[0] // HEAD
    rows = HEAD // pieces
    marks = []
    for h in range(heads):
        at = heads * HEAD + h
        a = keep_ref[at : at + 1, :] * got_ref[at : at + 1, :]
        high = a.astype(BF16).astype(F32)
        middle = (a - high).astype(BF16).astype(F32)
        low = a - high - middle
        marks += [high, middle, low]
    used = heads * rows
    marks.append(jnp.zeros((out_ref.shape[1] - used - len(marks), LANES), F32))
    marks = jnp.concatenate(marks, axis=0).astype(BF16)
    for z in range(pieces):
        parts = []
        for h in range(heads):
            at = heads * HEAD + h
            cut = slice(h * HEAD + z * rows, h * HEAD + (z + 1) * rows)
            parts.append(keep_ref[cut, :] * got_ref[at : at + 1, :] + got_ref[cut, :])
        out_ref[z, 0:used, :] = jnp.concatenate(parts, axis=0).astype(BF16)
        out_ref[z, used:, :] = marks


def scan_states(in_ref, out_ref):
    pieces, used, _ = out_ref.shape
    first = lax.axis_index("c") == 0
    half = used // 2
    state = jnp.zeros((used, LANES), F32)
    for t in range(pieces):
        j = jnp.where(first, t, pieces - 1 - t)
        part = in_ref[j].astype(F32)
        out_ref[j] = state.astype(BF16)
        decay = [
            jnp.sum(part[used + 3 * h : used + 3 * h + 3, :], axis=0, keepdims=True)
            for h in range(2)
        ]
        decay = jnp.concatenate([jnp.broadcast_to(d, (half, LANES)) for d in decay], axis=0)
        state = state * decay + part[:used, :]


def spread_states(in_ref, keep_ref, own_ref, send_ref):
    pieces, used, _ = in_ref.shape
    heads = own_ref.shape[0] // HEAD
    rows = used // heads
    for h in range(heads):
        at = heads * HEAD + h
        state = jnp.concatenate(
            [in_ref[z].astype(F32)[h * rows : (h + 1) * rows, :] for z in range(pieces)], axis=0
        )
        cut = slice(h * HEAD, (h + 1) * HEAD)
        own_ref[cut, :] = state.astype(BF16)
        send_ref[cut, :] = (state * keep_ref[at : at + 1, :] + keep_ref[cut, :]).astype(BF16)


def group_norm(values):
    centre = values - jnp.mean(values, axis=1, keepdims=True)
    spread = jnp.mean(centre * centre, axis=1, keepdims=True)
    return centre * lax.rsqrt(spread + GROUP_EPS)


def mix(inner_ref, query_ref, own_ref, got_ref, gated_ref, out_ref):
    heads = inner_ref.shape[2] // HEAD
    first = lax.axis_index("c") == 0
    mixed = []
    for h in range(heads):
        cut = slice(h * HEAD, (h + 1) * HEAD)
        own, got = own_ref[cut, :], got_ref[cut, :]
        combined = 0.0
        for way in range(2):
            state = jnp.where(first, own, got) if way == 0 else jnp.where(first, got, own)
            values = inner_ref[way, :, cut] + dot(query_ref[way, :, cut], state)
            combined = combined + group_norm(values) * gated_ref[way, :, cut]
        mixed.append(combined.astype(BF16))
    mixed = jnp.concatenate(mixed, axis=1)
    for p in range(out_ref.shape[0]):
        out_ref[p] = mixed


def project(pair, tp, *refs):
    mixed_ref, weight_ref, *refs = refs
    near, refs = refs[: tp - 1], refs[tp - 1 :]
    far, refs = refs[: tp - 1], refs[tp - 1 :]
    residuals, refs = refs[:pair], refs[pair:]
    gain_ref, normed_ref, middle_ref, first_ref, last_ref, scratch, table, spans, sems = refs
    me, member, core = lax.axis_index("tp"), lax.axis_index("pr"), lax.axis_index("c")
    n, width = mixed_ref.shape[1:]
    half = width // 2
    low = pl.multiple_of(core * half, half)
    high = pl.multiple_of((1 - core) * half, half)
    pairs = [(weight_ref, table.at[0])]
    for d in range(1, tp):
        pairs.append((near[d - 1], table.at[d, pl.ds(0, half)]))
        pairs.append((far[d - 1], table.at[d, pl.ds(half, half)]))
    pairs += [(residuals[s], spans.at[s]) for s in range(pair)]
    copies = fetch(pairs, sems)
    attended = 0.0
    for d in range(tp):
        parts = []
        for s in range(pair):
            i = lax.rem(member + s, pair) * tp + lax.rem(me - d + tp, tp)
            if d == 0:
                parts.append(mixed_ref[i])
            else:
                parts.append(
                    jnp.concatenate(
                        [mixed_ref[i, :, pl.ds(low, half)], mixed_ref[i, :, pl.ds(high, half)]],
                        axis=1,
                    )
                )
        for copy in copies[max(2 * d - 1, 0) : 2 * d + 1]:
            copy.wait()
        attended = attended + dot(jnp.concatenate(parts, axis=0), table[d])
    for copy in copies[2 * tp - 1 :]:
        copy.wait()
    firsts, lasts = [], []
    for s in range(pair):
        part = attended[s * n : (s + 1) * n, :]
        middle = (spans[s].astype(F32) + part).astype(BF16)
        if s == 0:
            scratch[...] = middle
        values = middle.astype(F32)
        scale = lax.rsqrt(jnp.mean(values * values, axis=1, keepdims=True) + NORM_EPS)
        normed = values * scale * gain_ref[...].astype(F32)
        normed_ref[s * n : (s + 1) * n, :] = normed.astype(BF16)
        firsts.append(normed[0:1, :])
        lasts.append(normed[n - 1 : n, :])
    own = middle_ref.shape[0]
    middle_ref[...] = scratch[pl.ds(pl.multiple_of(me * own, own), own), :]
    fill = [jnp.zeros((first_ref.shape[0] - pair, first_ref.shape[1]), F32)]
    first_ref[...] = jnp.concatenate(firsts + fill, axis=0).astype(BF16)
    last_ref[...] = jnp.concatenate(lasts + fill, axis=0).astype(BF16)


def convolved(pre, pair, taps):
    n = (pre.shape[0] - 16) // pair
    row = lax.broadcasted_iota(jnp.int32, (n, pre.shape[1]), 0)
    spans = []
    for s in range(pair):
        x = pre[s * n : (s + 1) * n, :]
        at = pair * n + s
        before = jnp.where(row == 0, pre[at : at + 1, :], pltpu.roll(x, 1, 0))
        after = jnp.where(row == n - 1, pre[at + 8 : at + 9, :], pltpu.roll(x, n - 1, 0))
        spans.append(taps[0:1] * before + taps[1:2] * x + taps[2:3] * after)
    return jnp.concatenate(spans, axis=0)


def feed_forward(pair, tp, ahead, *refs):
    sources, table_ref, refs = refs[:5], refs[5], refs[6:]
    outs, refs = refs[: pair * tp], refs[pair * tp :]
    (before_ref, after_ref, gt_ref, ut_ref, rows_ref, into, back), refs = refs[:7], refs[7:]
    hidden_ref, *sems = refs
    _, blocks, _, block = table_ref.shape
    steps = blocks // 3
    count, depth = sources[0].shape
    small = fetch(
        [
            *zip(sources[1:], (before_ref, after_ref, gt_ref, ut_ref)),
            (sources[0], rows_ref.at[pl.ds(0, count), :]),
        ],
        sems[0],
    )
    order = [i * steps + j for j in range(steps) for i in range(2)]
    order += [2 * steps + j for j in range(steps)]
    place = lambda i: pl.ds(i * block, block)
    copies = []
    for k in order:
        i, j = k // steps, k % steps
        target = into.at[j, :, :, place(i)] if i < 2 else back.at[:, :, place(j)]
        copies.append(pltpu.make_async_copy(table_ref.at[:, k], target, sems[1].at[k]))
    for copy in copies[:ahead]:
        copy.start()
    for copy in small:
        copy.wait()
    rows_ref[count:, :] = jnp.concatenate([before_ref[...], after_ref[...]], axis=0)
    cols, step = split_columns(pair, gt_ref.shape[1])
    member = lax.axis_index("pr")

    def arrive(first, last):
        for i in range(first, last):
            copies[i].wait()
            if i + ahead < len(copies):
                copies[i + ahead].start()

    for j in range(steps):
        at = pl.multiple_of(member * step + j * block, LANES)
        column = at + lax.broadcasted_iota(jnp.int32, (1, block), 1)
        up_taps = jnp.where(column >= member * cols, ut_ref[:, pl.ds(at, block)].astype(F32), 0.0)
        taps = jnp.concatenate([gt_ref[:, pl.ds(at, block)].astype(F32), up_taps], axis=1)
        arrive(2 * j, 2 * j + 2)
        pre = dot(rows_ref[...], into[j].reshape(depth, 2 * block)).astype(BF16).astype(F32)
        both = convolved(pre, pair, taps)
        hidden_ref[:, place(j)] = (silu(both[:, :block]) * both[:, block:]).astype(BF16)
    rows = outs[0].shape[0]
    me = lax.axis_index("tp")
    starts = [(s * tp + lax.rem(me + d, tp)) * rows for s in range(pair) for d in range(tp)]
    hidden = [hidden_ref[pl.ds(pl.multiple_of(at, rows), rows), :] for at in starts]
    arrive(2 * steps, 3 * steps)
    whole = back[...].reshape(depth, steps * block)
    part = dot(jnp.concatenate(hidden, axis=0), whole, ((1,), (1,)))
    for i, out_ref in enumerate(outs):
        out_ref[...] = part[i * rows : (i + 1) * rows, :].astype(BF16)


def run_feed_forward(pair, tp, normed, before, after, gathered, gate_taps, up_taps, ahead=6):
    spans, blocks, height, block = gathered.shape
    steps = blocks // 3
    rows, depth = normed.shape
    sources = (normed, before, after, gate_taps, up_taps)
    return call(
        lambda *refs: feed_forward(pair, tp, ahead, *refs),
        (near_by((rows // (pair * tp), depth), BF16),) * (pair * tp),
        *sources,
        gathered,
        limit=55,
        in_specs=[HBM] * 6,
        scratch_shapes=[pltpu.VMEM(a.shape, a.dtype) for a in sources[1:]]
        + [
            pltpu.VMEM((rows + 16, depth), BF16),
            pltpu.VMEM((steps, spans, height, 2 * block), BF16),
            pltpu.VMEM((spans, height, steps * block), BF16),
            pltpu.VMEM((rows, steps * block), BF16),
            pltpu.SemaphoreType.DMA((5,)),
            pltpu.SemaphoreType.DMA((blocks,)),
        ],
    )


def add_up(*refs):
    refs, out_ref = refs[:-1], refs[-1]
    total = refs[0][...].astype(F32)
    for ref in refs[1:]:
        total = total + ref[...].astype(F32)
    out_ref[...] = total.astype(BF16)


def across(x, axes):
    return lax.all_to_all(x, axes, 0, 0, tiled=True)


def shards(
    query_rows,
    key_rows,
    value_rows,
    gate_rows,
    log_decay,
    head_gain,
    out_weight,
    residual,
    norm_gain,
    gate_weight,
    up_weight,
    down_weight,
    gate_taps,
    up_taps,
):
    pair, chips, tp = lax.axis_size("pr"), lax.axis_size("z"), lax.axis_size("tp")
    peers = pair * tp
    rows, width = query_rows.shape
    depth = residual.shape[1]
    heads = width // HEAD
    cols, _ = split_columns(pair, gate_weight.shape[1])

    blocks = 3 * cols // BLOCK
    picked = call(
        lambda *refs: pick_weights(pair, *refs),
        shaped((blocks, gate_weight.shape[0], BLOCK), BF16),
        gate_weight,
        up_weight,
        down_weight,
        limit=60,
        in_specs=[HBM] * 3,
        out_specs=HBM,
        scratch_shapes=[pltpu.VMEM((blocks, gate_weight.shape[0], BLOCK), BF16)]
        + [pltpu.SemaphoreType.DMA((blocks,))] * 2,
    )
    gathered = lax.all_gather(picked, SP, axis=0, tiled=False)

    marked = near_by((heads * HEAD + 8, HEAD), F32)
    inputs = (query_rows, key_rows, value_rows, gate_rows, log_decay, head_gain)
    inner, query, gated, keep, send, half = call(
        local_retention,
        (
            near_by((2, rows, width), F32),
            near_by((2, rows, width), BF16),
            near_by((2, rows, width), F32),
            marked,
            marked,
            shaped((width // 2, depth), BF16),
        ),
        *inputs,
        out_weight,
        limit=60,
        in_specs=[HBM] * 7,
        scratch_shapes=[pltpu.VMEM(a.shape, a.dtype) for a in inputs]
        + [pltpu.SemaphoreType.DMA((7,))],
    )
    swap = [(0, 1), (1, 0)]
    got = lax.ppermute(send, "c", swap)
    near, far, residuals = [], [], [residual]
    for d in range(1, tp):
        near.append(lax.ppermute(half, "tp", [(i, (i + d) % tp) for i in range(tp)]))
    for a in near:
        far.append(lax.ppermute(a, "c", swap))
    for s in range(1, pair):
        residuals.append(lax.ppermute(residual, "pr", [((i + s) % pair, i) for i in range(pair)]))
    used = heads * HEAD // chips
    message = call(pack_states, near_by((chips, used + 8, HEAD), BF16), keep, got)
    arrived = across(message, "z")
    prefix = call(scan_states, near_by((chips, used, HEAD), BF16), arrived)
    returned = across(prefix, "z")
    state = near_by((heads * HEAD, HEAD), BF16)
    own, other = call(spread_states, (state, state), returned, keep)
    entering = lax.ppermute(other, "c", swap)
    shape = near_by((peers, rows, width), BF16)
    mixed = call(mix, shape, inner, query, own, entering, gated)
    edge = near_by((8, depth), BF16)
    normed, middle, first, last = call(
        lambda *refs: project(pair, tp, *refs),
        (near_by((pair * rows, depth), BF16), near_by((rows // tp, depth), BF16), edge, edge),
        across(mixed, PEERS),
        out_weight,
        *near,
        *far,
        *residuals,
        norm_gain.reshape(1, depth),
        limit=60,
        in_specs=[VMEM] + [HBM] * (2 * tp - 1 + pair) + [VMEM],
        scratch_shapes=[
            pltpu.VMEM((rows, depth), BF16),
            pltpu.VMEM((tp, width, depth), BF16),
            pltpu.VMEM((pair, rows, depth), BF16),
            pltpu.SemaphoreType.DMA((2 * tp - 1 + pair,)),
        ],
    )
    size = lax.axis_size("z") * lax.axis_size("c")
    onward = [(i, i + 1) for i in range(size - 1)]
    before = lax.ppermute(last, SP, onward)
    after = lax.ppermute(first, SP, [(j, i) for i, j in onward])
    parts = run_feed_forward(pair, tp, normed, before, after, gathered, gate_taps, up_taps)

    def collected(s):
        return [
            lax.ppermute(parts[s * tp + d], "tp", [(i, (i + d) % tp) for i in range(tp)])
            for d in range(1, tp)
        ]

    piece = (rows // tp, depth)
    sums = []
    for s in range(1, pair):
        arrived = collected(s)
        summed = call(add_up, near_by(piece, BF16), parts[s * tp], *arrived)
        sums.append(lax.ppermute(summed, "pr", [(i, (i + s) % pair) for i in range(pair)]))
    own_parts = collected(0)
    return call(add_up, shaped(piece, BF16), middle, parts[0], *own_parts, *sums)


def solution(mesh):
    groups, tp = mesh.shape["grp"], mesh.shape["tp"]
    pair = math.gcd(groups, 2)
    split = Mesh(
        mesh.devices.reshape(groups // pair, pair, mesh.shape["sp"] // 2, 2, tp),
        ("pg", "pr", "z", "c", "tp"),
    )
    placed = (
        P(ROWS, "tp"),
        P(ROWS, "tp"),
        P(ROWS, "tp"),
        P(ROWS, "tp"),
        P(None, "tp", ROWS),
        P(None, "tp"),
        P("tp", None),
        P(ROWS, None),
        P(),
        P(SP, "tp"),
        P(SP, "tp"),
        P(SP, "tp"),
        P(None, "tp"),
        P(None, "tp"),
    )

    return jax.shard_map(
        shards, mesh=split, in_specs=placed, out_specs=P((*ROWS, "tp"), None), check_vma=False
    )
```

```python
import math

import jax
import jax.numpy as jnp
from jax import lax
from jax.experimental import pallas as pl
from jax.experimental.pallas import tpu as pltpu
from jax.sharding import Mesh
from jax.sharding import PartitionSpec as P


HEAD = 128
LANES = 128
SP = ("z", "c")
ROWS = ("pg", "pr", "z", "c")
PEERS = ("pr", "tp")

GROUP_EPS = 1e-05
NORM_EPS = 1e-06


F32 = jnp.float32
BF16 = jnp.bfloat16
VMEM = pl.BlockSpec(memory_space=pltpu.VMEM)
HBM = pl.BlockSpec(memory_space=pltpu.HBM)
BLOCK = 256


def call(body, outs, *args, limit=12, **more):
    spec = {"in_specs": [VMEM] * len(args), "out_specs": jax.tree.map(lambda _: VMEM, outs)}
    return pl.pallas_call(
        body,
        out_shape=outs,
        compiler_params=pltpu.CompilerParams(vmem_limit_bytes=limit << 20),
        **{**spec, **more},
    )(*args)


def shaped(shape, dtype):
    return jax.ShapeDtypeStruct(shape, dtype)


def near_by(shape, dtype):
    return pltpu.VMEM(shape, dtype)


def dot(a, b, dims=((1,), (0,))):
    return lax.dot_general(a, b, (dims, ((), ())), preferred_element_type=F32)


def split_columns(pair, width):
    tiles = width // LANES
    share = -(-tiles // pair)
    step = (tiles - share) // (pair - 1) if pair > 1 else 0
    return share * LANES, step * LANES


def pick_weights(pair, gate_ref, up_ref, down_ref, out_ref, held, arrived, left):
    cols, step = split_columns(pair, gate_ref.shape[1])
    start = pl.multiple_of(lax.axis_index("pr") * step, LANES)
    blocks = cols // BLOCK
    sources = [
        ref.at[:, pl.ds(start + j * BLOCK, BLOCK)]
        for ref in (gate_ref, up_ref, down_ref)
        for j in range(blocks)
    ]
    copies = fetch([(src, held.at[k]) for k, src in enumerate(sources)], arrived)
    sends = []
    for k, copy in enumerate(copies):
        copy.wait()
        sends.append(pltpu.make_async_copy(held.at[k], out_ref.at[k], left.at[k]))
        sends[-1].start()
    for send in sends:
        send.wait()


def fetch(pairs, sems):
    copies = [pltpu.make_async_copy(src, dst, sems.at[i]) for i, (src, dst) in enumerate(pairs)]
    for copy in copies:
        copy.start()
    return copies


def silu(u):
    return u / (1.0 + jnp.exp(-u))


def local_retention(*refs):
    sources, refs = refs[:6], refs[6:]
    weight_ref, inner_ref, query_ref, gated_ref, keep_ref, send_ref, half_ref, *refs = refs
    held, sems = refs[:6], refs[6]
    half = half_ref.shape[0]
    start = pl.multiple_of(lax.axis_index("c") * half, half)
    copies = fetch(
        [*zip(sources, held), (weight_ref.at[pl.ds(start, half), :], half_ref)], sems
    )
    for copy in copies[:6]:
        copy.wait()
    q_ref, k_ref, v_ref, gate_ref, rate_ref, gain_ref = held
    n, width = q_ref.shape
    heads = width // HEAD
    row = lax.broadcasted_iota(jnp.int32, (n, n), 0)
    col = lax.broadcasted_iota(jnp.int32, (n, n), 1)
    scale = HEAD ** (-0.5)
    first = lax.axis_index("c") == 0
    gated = silu(gate_ref[...].astype(F32))
    for way in range(2):
        gated_ref[way] = gated * gain_ref[way : way + 1, :]
    for h in range(heads):
        cut = slice(h * HEAD, (h + 1) * HEAD)
        q, k, v = q_ref[:, cut], k_ref[:, cut], v_ref[:, cut]
        scores = dot(q, k, ((1,), (1,))) * scale
        states, decays = [], []
        for way in range(2):
            rate = rate_ref[way, h : h + 1, :]
            rate_col = jnp.sum(jnp.where(row == col, rate, 0.0), axis=1, keepdims=True)
            seen = col <= row if way == 0 else col >= row
            seen_by = row <= col if way == 0 else row >= col
            total_col = jnp.sum(jnp.where(seen, rate, 0.0), axis=1, keepdims=True)
            total_row = jnp.sum(jnp.where(seen_by, rate_col, 0.0), axis=0, keepdims=True)
            whole = jnp.sum(rate, axis=1, keepdims=True)
            mask = jnp.where(seen, jnp.exp(jnp.minimum(total_col - total_row, 0.0)), 0.0)
            inner_ref[way, :, cut] = dot((scores * mask).astype(BF16), v)
            query_ref[way, :, cut] = (q.astype(F32) * jnp.exp(total_col)).astype(BF16)
            weight = jnp.exp(whole - total_col) * scale
            states.append(dot((k.astype(F32) * weight).astype(BF16), v, ((0,), (0,))))
            decays.append(jnp.broadcast_to(jnp.exp(whole), (1, HEAD)))
        rows = slice(h * HEAD, (h + 1) * HEAD)
        keep_ref[rows, :] = jnp.where(first, states[0], states[1])
        send_ref[rows, :] = jnp.where(first, states[1], states[0])
        mark = slice(heads * HEAD + h, heads * HEAD + h + 1)
        keep_ref[mark, :] = jnp.where(first, decays[0], decays[1])
        send_ref[mark, :] = jnp.where(first, decays[1], decays[0])
    copies[6].wait()


def pack_states(keep_ref, got_ref, out_ref):
    pieces = out_ref.shape[0]
    heads = keep_ref.shape[0] // HEAD
    rows = HEAD // pieces
    marks = []
    for h in range(heads):
        at = heads * HEAD + h
        a = keep_ref[at : at + 1, :] * got_ref[at : at + 1, :]
        high = a.astype(BF16).astype(F32)
        middle = (a - high).astype(BF16).astype(F32)
        low = a - high - middle
        marks += [high, middle, low]
    used = heads * rows
    marks.append(jnp.zeros((out_ref.shape[1] - used - len(marks), LANES), F32))
    marks = jnp.concatenate(marks, axis=0).astype(BF16)
    for z in range(pieces):
        parts = []
        for h in range(heads):
            at = heads * HEAD + h
            cut = slice(h * HEAD + z * rows, h * HEAD + (z + 1) * rows)
            parts.append(keep_ref[cut, :] * got_ref[at : at + 1, :] + got_ref[cut, :])
        out_ref[z, 0:used, :] = jnp.concatenate(parts, axis=0).astype(BF16)
        out_ref[z, used:, :] = marks


def scan_states(in_ref, out_ref):
    pieces, used, _ = out_ref.shape
    first = lax.axis_index("c") == 0
    half = used // 2
    state = jnp.zeros((used, LANES), F32)
    for t in range(pieces):
        j = jnp.where(first, t, pieces - 1 - t)
        part = in_ref[j].astype(F32)
        out_ref[j] = state.astype(BF16)
        decay = [
            jnp.sum(part[used + 3 * h : used + 3 * h + 3, :], axis=0, keepdims=True)
            for h in range(2)
        ]
        decay = jnp.concatenate([jnp.broadcast_to(d, (half, LANES)) for d in decay], axis=0)
        state = state * decay + part[:used, :]


def spread_states(in_ref, keep_ref, own_ref, send_ref):
    pieces, used, _ = in_ref.shape
    heads = own_ref.shape[0] // HEAD
    rows = used // heads
    for h in range(heads):
        at = heads * HEAD + h
        state = jnp.concatenate(
            [in_ref[z].astype(F32)[h * rows : (h + 1) * rows, :] for z in range(pieces)], axis=0
        )
        cut = slice(h * HEAD, (h + 1) * HEAD)
        own_ref[cut, :] = state.astype(BF16)
        send_ref[cut, :] = (state * keep_ref[at : at + 1, :] + keep_ref[cut, :]).astype(BF16)


def group_norm(values):
    centre = values - jnp.mean(values, axis=1, keepdims=True)
    spread = jnp.mean(centre * centre, axis=1, keepdims=True)
    return centre * lax.rsqrt(spread + GROUP_EPS)


def mix(inner_ref, query_ref, own_ref, got_ref, gated_ref, out_ref):
    heads = inner_ref.shape[2] // HEAD
    first = lax.axis_index("c") == 0
    mixed = []
    for h in range(heads):
        cut = slice(h * HEAD, (h + 1) * HEAD)
        own, got = own_ref[cut, :], got_ref[cut, :]
        combined = 0.0
        for way in range(2):
            state = jnp.where(first, own, got) if way == 0 else jnp.where(first, got, own)
            values = inner_ref[way, :, cut] + dot(query_ref[way, :, cut], state)
            combined = combined + group_norm(values) * gated_ref[way, :, cut]
        mixed.append(combined.astype(BF16))
    mixed = jnp.concatenate(mixed, axis=1)
    for p in range(out_ref.shape[0]):
        out_ref[p] = mixed


def project(pair, tp, *refs):
    mixed_ref, weight_ref, *refs = refs
    near, refs = refs[: tp - 1], refs[tp - 1 :]
    far, refs = refs[: tp - 1], refs[tp - 1 :]
    residuals, refs = refs[:pair], refs[pair:]
    gain_ref, normed_ref, middle_ref, first_ref, last_ref, scratch, table, spans, sems = refs
    me, member, core = lax.axis_index("tp"), lax.axis_index("pr"), lax.axis_index("c")
    n, width = mixed_ref.shape[1:]
    half = width // 2
    low = pl.multiple_of(core * half, half)
    high = pl.multiple_of((1 - core) * half, half)
    pairs = [(weight_ref, table.at[0])]
    for d in range(1, tp):
        pairs.append((near[d - 1], table.at[d, pl.ds(0, half)]))
        pairs.append((far[d - 1], table.at[d, pl.ds(half, half)]))
    pairs += [(residuals[s], spans.at[s]) for s in range(pair)]
    copies = fetch(pairs, sems)
    attended = 0.0
    for d in range(tp):
        parts = []
        for s in range(pair):
            i = lax.rem(member + s, pair) * tp + lax.rem(me - d + tp, tp)
            if d == 0:
                parts.append(mixed_ref[i])
            else:
                parts.append(
                    jnp.concatenate(
                        [mixed_ref[i, :, pl.ds(low, half)], mixed_ref[i, :, pl.ds(high, half)]],
                        axis=1,
                    )
                )
        for copy in copies[max(2 * d - 1, 0) : 2 * d + 1]:
            copy.wait()
        attended = attended + dot(jnp.concatenate(parts, axis=0), table[d])
    for copy in copies[2 * tp - 1 :]:
        copy.wait()
    firsts, lasts = [], []
    for s in range(pair):
        part = attended[s * n : (s + 1) * n, :]
        middle = (spans[s].astype(F32) + part).astype(BF16)
        if s == 0:
            scratch[...] = middle
        values = middle.astype(F32)
        scale = lax.rsqrt(jnp.mean(values * values, axis=1, keepdims=True) + NORM_EPS)
        normed = values * scale * gain_ref[...].astype(F32)
        normed_ref[s * n : (s + 1) * n, :] = normed.astype(BF16)
        firsts.append(normed[0:1, :])
        lasts.append(normed[n - 1 : n, :])
    own = middle_ref.shape[0]
    middle_ref[...] = scratch[pl.ds(pl.multiple_of(me * own, own), own), :]
    fill = [jnp.zeros((first_ref.shape[0] - pair, first_ref.shape[1]), F32)]
    first_ref[...] = jnp.concatenate(firsts + fill, axis=0).astype(BF16)
    last_ref[...] = jnp.concatenate(lasts + fill, axis=0).astype(BF16)


def convolved(pre, pair, taps):
    n = (pre.shape[0] - 16) // pair
    row = lax.broadcasted_iota(jnp.int32, (n, pre.shape[1]), 0)
    spans = []
    for s in range(pair):
        x = pre[s * n : (s + 1) * n, :]
        at = pair * n + s
        before = jnp.where(row == 0, pre[at : at + 1, :], pltpu.roll(x, 1, 0))
        after = jnp.where(row == n - 1, pre[at + 8 : at + 9, :], pltpu.roll(x, n - 1, 0))
        spans.append(taps[0:1] * before + taps[1:2] * x + taps[2:3] * after)
    return jnp.concatenate(spans, axis=0)


def feed_forward(pair, tp, ahead, *refs):
    sources, table_ref, refs = refs[:5], refs[5], refs[6:]
    outs, refs = refs[: pair * tp], refs[pair * tp :]
    (before_ref, after_ref, gt_ref, ut_ref, rows_ref, into, back), refs = refs[:7], refs[7:]
    hidden_ref, *sems = refs
    _, blocks, _, block = table_ref.shape
    steps = blocks // 3
    count, depth = sources[0].shape
    small = fetch(
        [
            *zip(sources[1:], (before_ref, after_ref, gt_ref, ut_ref)),
            (sources[0], rows_ref.at[pl.ds(0, count), :]),
        ],
        sems[0],
    )
    order = [i * steps + j for j in range(steps) for i in range(2)]
    order += [2 * steps + j for j in range(steps)]
    place = lambda i: pl.ds(i * block, block)
    copies = []
    for k in order:
        i, j = k // steps, k % steps
        target = into.at[j, :, :, place(i)] if i < 2 else back.at[:, :, place(j)]
        copies.append(pltpu.make_async_copy(table_ref.at[:, k], target, sems[1].at[k]))
    for copy in copies[:ahead]:
        copy.start()
    for copy in small:
        copy.wait()
    rows_ref[count:, :] = jnp.concatenate([before_ref[...], after_ref[...]], axis=0)
    cols, step = split_columns(pair, gt_ref.shape[1])
    member = lax.axis_index("pr")

    def arrive(first, last):
        for i in range(first, last):
            copies[i].wait()
            if i + ahead < len(copies):
                copies[i + ahead].start()

    for j in range(steps):
        at = pl.multiple_of(member * step + j * block, LANES)
        column = at + lax.broadcasted_iota(jnp.int32, (1, block), 1)
        up_taps = jnp.where(column >= member * cols, ut_ref[:, pl.ds(at, block)].astype(F32), 0.0)
        taps = jnp.concatenate([gt_ref[:, pl.ds(at, block)].astype(F32), up_taps], axis=1)
        arrive(2 * j, 2 * j + 2)
        pre = dot(rows_ref[...], into[j].reshape(depth, 2 * block)).astype(BF16).astype(F32)
        both = convolved(pre, pair, taps)
        hidden_ref[:, place(j)] = (silu(both[:, :block]) * both[:, block:]).astype(BF16)
    rows = outs[0].shape[0]
    me = lax.axis_index("tp")
    starts = [(s * tp + lax.rem(me + d, tp)) * rows for s in range(pair) for d in range(tp)]
    hidden = [hidden_ref[pl.ds(pl.multiple_of(at, rows), rows), :] for at in starts]
    arrive(2 * steps, 3 * steps)
    whole = back[...].reshape(depth, steps * block)
    part = dot(jnp.concatenate(hidden, axis=0), whole, ((1,), (1,)))
    for i, out_ref in enumerate(outs):
        out_ref[...] = part[i * rows : (i + 1) * rows, :].astype(BF16)


def run_feed_forward(pair, tp, normed, before, after, gathered, gate_taps, up_taps, ahead=6):
    spans, blocks, height, block = gathered.shape
    steps = blocks // 3
    rows, depth = normed.shape
    sources = (normed, before, after, gate_taps, up_taps)
    return call(
        lambda *refs: feed_forward(pair, tp, ahead, *refs),
        (near_by((rows // (pair * tp), depth), BF16),) * (pair * tp),
        *sources,
        gathered,
        limit=55,
        in_specs=[HBM] * 6,
        scratch_shapes=[pltpu.VMEM(a.shape, a.dtype) for a in sources[1:]]
        + [
            pltpu.VMEM((rows + 16, depth), BF16),
            pltpu.VMEM((steps, spans, height, 2 * block), BF16),
            pltpu.VMEM((spans, height, steps * block), BF16),
            pltpu.VMEM((rows, steps * block), BF16),
            pltpu.SemaphoreType.DMA((5,)),
            pltpu.SemaphoreType.DMA((blocks,)),
        ],
    )


def add_up(*refs):
    refs, out_ref = refs[:-1], refs[-1]
    total = refs[0][...].astype(F32)
    for ref in refs[1:]:
        total = total + ref[...].astype(F32)
    out_ref[...] = total.astype(BF16)


def across(x, axes):
    return lax.all_to_all(x, axes, 0, 0, tiled=True)


def shards(
    query_rows,
    key_rows,
    value_rows,
    gate_rows,
    log_decay,
    head_gain,
    out_weight,
    residual,
    norm_gain,
    gate_weight,
    up_weight,
    down_weight,
    gate_taps,
    up_taps,
):
    pair, chips, tp = lax.axis_size("pr"), lax.axis_size("z"), lax.axis_size("tp")
    peers = pair * tp
    rows, width = query_rows.shape
    depth = residual.shape[1]
    heads = width // HEAD
    cols, _ = split_columns(pair, gate_weight.shape[1])

    blocks = 3 * cols // BLOCK
    picked = call(
        lambda *refs: pick_weights(pair, *refs),
        shaped((blocks, gate_weight.shape[0], BLOCK), BF16),
        gate_weight,
        up_weight,
        down_weight,
        limit=60,
        in_specs=[HBM] * 3,
        out_specs=HBM,
        scratch_shapes=[pltpu.VMEM((blocks, gate_weight.shape[0], BLOCK), BF16)]
        + [pltpu.SemaphoreType.DMA((blocks,))] * 2,
    )
    gathered = lax.all_gather(picked, SP, axis=0, tiled=False)

    marked = near_by((heads * HEAD + 8, HEAD), F32)
    inputs = (query_rows, key_rows, value_rows, gate_rows, log_decay, head_gain)
    inner, query, gated, keep, send, half = call(
        local_retention,
        (
            near_by((2, rows, width), F32),
            near_by((2, rows, width), BF16),
            near_by((2, rows, width), F32),
            marked,
            marked,
            shaped((width // 2, depth), BF16),
        ),
        *inputs,
        out_weight,
        limit=60,
        in_specs=[HBM] * 7,
        scratch_shapes=[pltpu.VMEM(a.shape, a.dtype) for a in inputs]
        + [pltpu.SemaphoreType.DMA((7,))],
    )
    swap = [(0, 1), (1, 0)]
    got = lax.ppermute(send, "c", swap)
    near, far, residuals = [], [], [residual]
    for d in range(1, tp):
        near.append(lax.ppermute(half, "tp", [(i, (i + d) % tp) for i in range(tp)]))
    for a in near:
        far.append(lax.ppermute(a, "c", swap))
    for s in range(1, pair):
        residuals.append(lax.ppermute(residual, "pr", [((i + s) % pair, i) for i in range(pair)]))
    used = heads * HEAD // chips
    message = call(pack_states, near_by((chips, used + 8, HEAD), BF16), keep, got)
    arrived = across(message, "z")
    prefix = call(scan_states, near_by((chips, used, HEAD), BF16), arrived)
    returned = across(prefix, "z")
    state = near_by((heads * HEAD, HEAD), BF16)
    own, other = call(spread_states, (state, state), returned, keep)
    entering = lax.ppermute(other, "c", swap)
    shape = near_by((peers, rows, width), BF16)
    mixed = call(mix, shape, inner, query, own, entering, gated)
    edge = near_by((8, depth), BF16)
    normed, middle, first, last = call(
        lambda *refs: project(pair, tp, *refs),
        (near_by((pair * rows, depth), BF16), near_by((rows // tp, depth), BF16), edge, edge),
        across(mixed, PEERS),
        out_weight,
        *near,
        *far,
        *residuals,
        norm_gain.reshape(1, depth),
        limit=60,
        in_specs=[VMEM] + [HBM] * (2 * tp - 1 + pair) + [VMEM],
        scratch_shapes=[
            pltpu.VMEM((rows, depth), BF16),
            pltpu.VMEM((tp, width, depth), BF16),
            pltpu.VMEM((pair, rows, depth), BF16),
            pltpu.SemaphoreType.DMA((2 * tp - 1 + pair,)),
        ],
    )
    size = lax.axis_size("z") * lax.axis_size("c")
    onward = [(i, i + 1) for i in range(size - 1)]
    before = lax.ppermute(last, SP, onward)
    after = lax.ppermute(first, SP, [(j, i) for i, j in onward])
    parts = run_feed_forward(pair, tp, normed, before, after, gathered, gate_taps, up_taps)

    def collected(s):
        out = []
        for d in range(1, tp):
            peers_of = [(i, (i + d) % tp) for i in range(tp)]
            out.append(lax.ppermute(parts[s * tp + d], "tp", peers_of))
        return out

    piece = (rows // tp, depth)
    sums = []
    for s in range(1, pair):
        arrived = collected(s)
        summed = call(add_up, near_by(piece, BF16), parts[s * tp], *arrived)
        sums.append(lax.ppermute(summed, "pr", [(i, (i + s) % pair) for i in range(pair)]))
    own_parts = collected(0)
    return call(add_up, shaped(piece, BF16), middle, parts[0], *own_parts, *sums)


def solution(mesh):
    groups, tp = mesh.shape["grp"], mesh.shape["tp"]
    pair = math.gcd(groups, 2)
    split = Mesh(
        mesh.devices.reshape(groups // pair, pair, mesh.shape["sp"] // 2, 2, tp),
        ("pg", "pr", "z", "c", "tp"),
    )
    placed = (
        P(ROWS, "tp"),
        P(ROWS, "tp"),
        P(ROWS, "tp"),
        P(ROWS, "tp"),
        P(None, "tp", ROWS),
        P(None, "tp"),
        P("tp", None),
        P(ROWS, None),
        P(),
        P(SP, "tp"),
        P(SP, "tp"),
        P(SP, "tp"),
        P(None, "tp"),
        P(None, "tp"),
    )

    return jax.shard_map(
        shards, mesh=split, in_specs=placed, out_specs=P((*ROWS, "tp"), None), check_vma=False
    )
```
